1024 devices in a mesh: ep: 64 (over z, y), tp: 16 (over x, core).
Axes of the slice: x: 8, y: 8, z: 8, core: 2. Of those that a mesh axis runs over, the one named last changes fastest.
Arguments:
- tokens: bfloat16 [16384, 2048], P('ep', 'tp'), may hold values from -400 to 400
- expert_ids: int32 [16384, 2], P('ep'), may hold values from 0 to 63, all different within a row; in each aligned block of 256 rows (0 to 255, 256 to 511, ...) at most 10 rows name the same one
- route_weights: float32 [16384, 2], P('ep'), may hold values from 0.1 to 1
- pre_gain: float32 [2048], P('tp'), may hold values from 0.1 to 1.9
- post_gain: float32 [2048], P('tp'), may hold values from 0.1 to 1.9
- gate_weight: bfloat16 [64, 2048, 4096], P('ep', None, 'tp'), may hold values from -0.125 to 0.125
- up_weight: bfloat16 [64, 2048, 4096], P('ep', None, 'tp'), may hold values from -0.125 to 0.125
- down_weight: bfloat16 [64, 4096, 2048], P('ep', None, 'tp'), may hold values from -0.71875 to 0.71875
Outputs:
- layer_out: bfloat16 [16384, 2048], P('ep', 'tp')
The draws below stay inside these ranges and needn't reach their ends.
Inputs may be any that keep to these rules, and one draw needn't show every extreme that they name: `expert_ids`: the 2 experts of a token are distinct. Within the rows of one device along ep, no expert is named more than 10 times, a bound that some block reaches.
All inputs are finite; a program needn't handle non-finite values.
Results may differ from the reference program's by a relative error of at most 0.007.
Values may be sent and summed in bfloat16 or wider, within the bound.
No kernel may reach another device: no remote copies, remote signals or barrier semaphores. Data moves between devices by JAX's collectives and lax.ppermute only.
A program may use at most 64 MiB of HBM per device.

```python
import math
import jax
import jax.numpy as jnp
import numpy as np
from jax import lax

D = 2048
DE = 4096
TOPK = 2
TOK_DEV = 256
EXPERTS = 64
TOKENS = 16384
CAP = 10
N_EP = 64


def draw_tokens(key, part):
    first, second, third = jax.random.split(jax.random.fold_in(key, 11), 3)
    base = jnp.clip(jax.random.normal(first, (TOKENS, D), jnp.float32), -6.0, 6.0)
    rising = jnp.exp(jnp.log(4.0) * jnp.arange(D, dtype=jnp.float32) / D)
    rough = jax.random.uniform(second, (1, D), jnp.float32, 0.5, 1.5)
    row_scale = jnp.exp(jax.random.uniform(third, (TOKENS, 1), jnp.float32, 0.0, jnp.log(10.0)))
    return (base * rising[None, :] * rough * row_scale).astype(jnp.bfloat16)


def draw_down_weight(key, part):
    first, second = jax.random.split(jax.random.fold_in(key, 23), 2)
    base = jnp.clip(jax.random.normal(first, (EXPERTS, DE, D), jnp.float32), -6.0, 6.0)
    rising = jnp.exp(jnp.log(5.0) * jnp.arange(D, dtype=jnp.float32) / D)
    rough = jax.random.uniform(second, (1, 1, D), jnp.float32, 0.5, 1.5)
    return (base * rising[None, None, :] * rough * DE ** (-0.5)).astype(jnp.bfloat16)


def steps_of(stream_key, dims, cuts, smallest, top_value):
    level, own = 1.0, jax.random.fold_in(stream_key, 6)
    for axis_at, parts in cuts:
        steps = jnp.exp(jax.random.uniform(jax.random.fold_in(own, axis_at), (parts,), jnp.float32, smallest / len(cuts), top_value / len(cuts)))
        level = level * jnp.repeat(steps, dims[axis_at] // parts).reshape([-1 if axis == axis_at else 1 for axis in range(len(dims))])
    return level


def assign_block(key, own, number, rows, count, top, reach, skew):
    order = jax.random.permutation(key, count)
    packed, common = load_shares(count, rows * top, reach, skew, True), load_shares(count, rows * top, reach, skew, False)
    places = jnp.arange(count)

    def named(tallies, turn):
        used = int((tallies > 0).sum())
        fixed = max(1, used // 4)
        moved = fixed + (places - fixed + turn * (used - fixed)) % max(1, count - fixed)
        return jnp.zeros((count,), jnp.int32).at[order[jnp.where(places < fixed, places, moved)]].set(jnp.asarray(tallies, jnp.int32))

    tallies = jnp.where(number % 4 == 0, named(packed, number // 4), named(common, number - number // 4 - 1))
    mixed = jax.random.permutation(jax.random.fold_in(own, 3), count)
    giver, receiver = mixed[0:count // 2 * 2:2], mixed[1:count // 2 * 2:2]
    margin = jnp.minimum(tallies[giver] - 1, reach - tallies[receiver]) // 2
    margin = jnp.where((giver == order[0]) | (receiver == order[0]) | (tallies[receiver] == 0), 0, jnp.maximum(margin, 0))
    moved = jax.random.randint(jax.random.fold_in(own, 4), (count // 2,), 0, 1 << 20) % (margin + 1)
    tallies = tallies.at[giver].add(-moved).at[receiver].add(moved)
    items = jnp.searchsorted(jnp.cumsum(tallies), jnp.arange(rows * top), side="right").astype(jnp.int32)
    grid = items.reshape(top, rows).T
    grid = grid[jax.random.permutation(jax.random.fold_in(own, 1), rows)]
    turn = jax.random.randint(jax.random.fold_in(own, 2), (rows, 1), 0, top)
    return jnp.take_along_axis(grid, (jnp.arange(top)[None, :] + turn) % top, axis=1)


def load_shares(count, total, bound, skew, full):
    portions = [(1 << 20) // math.isqrt(standing ** skew) + 1 for standing in range(1, count + 1)]
    largest = bound if full else min(bound, max(-(-total // count), total * portions[0] // sum(portions)))
    least = 1 if total - largest >= count - 1 else 0
    given, spare = [largest] + [least] * (count - 1), total - largest - least * (count - 1)
    while spare > 0:
        free = [i for i in range(1, count) if given[i] < largest] or [i for i in range(1, count) if given[i] < bound]
        mass, remaining = sum([portions[i] for i in free]), spare
        for i in free:
            addition = min(bound - given[i], max(1, remaining * portions[i] // mass), spare)
            given[i] = given[i] + addition
            spare = spare - addition
    return np.array(given)


def bell_draw(own_key, extent, width, most, cuts=(), kind=jnp.bfloat16):
    result = width * jax.random.normal(own_key, extent, jnp.float32)
    if cuts:
        result = result * steps_of(own_key, extent, cuts, -0.22, 0.18)
    return jnp.clip(result, -most, most).astype(kind)


def setup_inputs(seed: int = 0) -> dict:
    streams_of = jax.random.split(jax.random.key(seed), 9)
    tokens = draw_tokens(jax.random.fold_in(streams_of[8], 71), 0)
    expert_ids_keys = jax.random.split(jax.random.fold_in(streams_of[1], 1), TOKENS // TOK_DEV)
    expert_ids_turns = jax.random.permutation(jax.random.fold_in(streams_of[1], 3), TOKENS // TOK_DEV)
    expert_ids = jax.vmap(lambda own, number: assign_block(jax.random.fold_in(streams_of[1], 2), own, number, TOK_DEV, EXPERTS, TOPK, CAP, 2))(expert_ids_keys, expert_ids_turns).reshape((TOKENS, TOPK))
    route_weights = jnp.clip(0.1 + 0.9 * jax.random.uniform(streams_of[2], (TOKENS, TOPK), jnp.float32) ** steps_of(streams_of[2], (TOKENS, TOPK), ((0, 64),), -0.2, 0.2), 0.1, 1.0)
    pre_gain = jnp.clip(1.0 + 0.18 * jax.random.normal(streams_of[3], (D,), jnp.float32), 0.1, 1.9)
    post_gain = jnp.clip(1.0 + 0.18 * jax.random.normal(streams_of[4], (D,), jnp.float32), 0.1, 1.9)
    gate_weight = bell_draw(streams_of[5], (EXPERTS, D, DE), D ** -0.5, 0.125, ((0, 64), (2, 16)))
    up_weight = bell_draw(streams_of[6], (EXPERTS, D, DE), D ** -0.5, 0.125, ((0, 64), (2, 16)))
    down_weight = draw_down_weight(jax.random.fold_in(streams_of[8], 71), 0)
    return {"tokens": tokens, "expert_ids": expert_ids, "route_weights": route_weights, "pre_gain": pre_gain, "post_gain": post_gain, "gate_weight": gate_weight, "up_weight": up_weight, "down_weight": down_weight}


epsilon = 1e-06

def reference(tokens, expert_ids, route_weights, pre_gain, post_gain, gate_weight, up_weight, down_weight):
    tok_float = tokens.astype(jnp.float32)
    mean_in = lax.optimization_barrier(jnp.mean(tok_float * tok_float, axis=1, keepdims=True))
    normed = (tok_float * lax.rsqrt(mean_in + epsilon) * pre_gain.astype(jnp.float32)[None, :]).astype(jnp.bfloat16)
    pairs = N_EP * TOK_DEV * TOPK
    blocks = expert_ids.reshape(N_EP, TOK_DEV * TOPK)
    onehot = (blocks[:, :, None] == jnp.arange(EXPERTS, dtype=jnp.int32)[None, None, :]).astype(jnp.int32)
    slot = lax.optimization_barrier(jnp.sum((jnp.cumsum(onehot, axis=1) - 1) * onehot, axis=2)).astype(jnp.int32).reshape(-1)
    block_of = jnp.arange(pairs, dtype=jnp.int32) // (TOK_DEV * TOPK)
    flat_ids = expert_ids.reshape(-1).astype(jnp.int32)
    row_of = (block_of * CAP + slot).astype(jnp.int32)
    token_of = jnp.arange(pairs, dtype=jnp.int32) // TOPK
    table = jnp.full((EXPERTS, N_EP * CAP), TOKENS, jnp.int32).at[flat_ids, row_of].set(token_of)
    padded = jnp.concatenate([normed, jnp.zeros((1, D), jnp.bfloat16)], axis=0)

    def expert(inputs):
        row_index, w_gate, w_up, w_down = inputs
        rows = padded[row_index].astype(jnp.float32)
        gate = jnp.dot(rows, w_gate.astype(jnp.float32))
        upper = jnp.dot(rows, w_up.astype(jnp.float32))
        hidden = (jax.nn.silu(gate) * upper).astype(jnp.bfloat16)
        return jnp.dot(hidden.astype(jnp.float32), w_down.astype(jnp.float32)).astype(jnp.bfloat16)
    results = lax.map(expert, (table, gate_weight, up_weight, down_weight))
    picked = results[flat_ids, row_of].reshape(TOKENS, TOPK, D).astype(jnp.float32)
    mixed = lax.optimization_barrier(jnp.sum(picked * route_weights.astype(jnp.float32)[:, :, None], axis=1))
    mean_out = lax.optimization_barrier(jnp.mean(mixed * mixed, axis=1, keepdims=True))
    return (mixed * lax.rsqrt(mean_out + epsilon) * post_gain.astype(jnp.float32)[None, :]).astype(jnp.bfloat16)
```

```python
import jax
import jax.numpy as jnp
from jax import lax
from jax.experimental import pallas as pl
from jax.experimental.pallas import tpu as pltpu
from jax.sharding import PartitionSpec as P

epsilon = 1e-06
PAD = 16
EXTRA = 16


def dispatch_kernel(tok_ref, ids_ref, weights_ref, out_ref, cols_ref):
    rows = tok_ref.shape[0]
    slots = out_ref.shape[0]
    experts = slots // PAD
    ids = ids_ref[...]
    expert_index = lax.broadcasted_iota(jnp.int32, (experts, rows), 0)
    hot0 = jnp.where(expert_index == ids[0:1, :], 1.0, 0.0)
    hot1 = jnp.where(expert_index == ids[1:2, :], 1.0, 0.0)
    earlier = lax.broadcasted_iota(jnp.int32, (rows, rows), 0) < lax.broadcasted_iota(
        jnp.int32, (rows, rows), 1
    )
    earlier = jnp.where(earlier, 1.0, 0.0).astype(jnp.bfloat16)
    counts = jnp.dot((hot0 + hot1).astype(jnp.bfloat16), earlier, preferred_element_type=jnp.float32)
    slot0 = jnp.sum(hot0 * counts, axis=0, keepdims=True)
    slot1 = jnp.sum(hot1 * counts, axis=0, keepdims=True)
    target0 = ids[0:1, :] * PAD + slot0.astype(jnp.int32)
    target1 = ids[1:2, :] * PAD + slot1.astype(jnp.int32)
    slot_index = lax.broadcasted_iota(jnp.int32, (slots, rows), 0)
    chosen = jnp.logical_or(slot_index == target0, slot_index == target1)
    chosen = jnp.where(chosen, 1.0, 0.0).astype(jnp.bfloat16)
    out_ref[...] = jnp.dot(chosen, tok_ref[...], preferred_element_type=jnp.float32).astype(
        jnp.bfloat16
    )
    weights = weights_ref[...]
    lines = jnp.concatenate(
        [
            target0.astype(jnp.float32),
            target1.astype(jnp.float32),
            weights,
            jnp.zeros((4, rows), jnp.float32),
        ],
        axis=0,
    )
    cols_ref[...] = jnp.transpose(lines)


def dispatch(tokens, ids, weights, slots):
    rows, width = tokens.shape
    return pl.pallas_call(
        dispatch_kernel,
        out_shape=(
            jax.ShapeDtypeStruct((slots, width), jnp.bfloat16),
            jax.ShapeDtypeStruct((rows, 8), jnp.float32),
        ),
        name="dispatch",
    )(tokens, ids, weights)


def hidden_kernel(feat_ref, gain_ref, gate_ref, up_ref, out_ref, normed_ref):
    parts, rows, width = feat_ref.shape
    full = parts * width
    total = jnp.zeros((rows, width), jnp.float32)
    for j in range(parts):
        part = feat_ref[j].astype(jnp.float32)
        total = total + part * part
    scale = lax.rsqrt(jnp.sum(total, axis=1, keepdims=True) / full + epsilon)
    for j in range(parts):
        pieces = gain_ref[j].astype(jnp.float32)
        gain = pieces[0:1, :] + pieces[1:2, :] + pieces[2:3, :]
        part = feat_ref[j].astype(jnp.float32)
        normed_ref[:, j * width : (j + 1) * width] = (part * scale * gain).astype(jnp.bfloat16)
    normed = normed_ref[...]
    gate = jnp.dot(normed, gate_ref[...], preferred_element_type=jnp.float32)
    upper = jnp.dot(normed, up_ref[...], preferred_element_type=jnp.float32)
    out_ref[...] = (gate / (1.0 + jnp.exp(-gate)) * upper).astype(jnp.bfloat16)


def hidden_of(features, gate_weight, up_weight, row_total, tile):
    parts, _, width = features.shape
    full, units = gate_weight.shape
    return pl.pallas_call(
        hidden_kernel,
        grid=(row_total // tile,),
        in_specs=[
            pl.BlockSpec((parts, tile, width), lambda i: (0, i, 0)),
            pl.BlockSpec((parts, EXTRA, width), lambda i: (0, row_total // EXTRA, 0)),
            pl.BlockSpec((full, units), lambda i: (0, 0)),
            pl.BlockSpec((full, units), lambda i: (0, 0)),
        ],
        out_specs=pl.BlockSpec((tile, units), lambda i: (i, 0)),
        out_shape=jax.ShapeDtypeStruct((row_total, units), jnp.bfloat16),
        scratch_shapes=[pltpu.VMEM((tile, full), jnp.bfloat16)],
        name="hidden",
    )(features, features, gate_weight, up_weight)


def down_kernel(hidden_ref, down_ref, out_ref):
    parts, rows, units = hidden_ref.shape
    blocks, _, width = out_ref.shape
    capacity = rows // blocks
    total = jnp.zeros((rows, width), jnp.float32)
    for j in range(parts):
        total = total + jnp.dot(
            hidden_ref[j],
            down_ref[j * units : (j + 1) * units, :],
            preferred_element_type=jnp.float32,
        )
    empty = jnp.zeros((PAD - capacity, width), jnp.float32)
    for b in range(blocks):
        block = jnp.concatenate([total[b * capacity : (b + 1) * capacity, :], empty], axis=0)
        out_ref[b] = block.astype(jnp.bfloat16)


def down_of(hidden, down_weight, blocks_total, tile_blocks):
    parts, row_total, units = hidden.shape
    full, width = down_weight.shape
    tile = row_total // blocks_total * tile_blocks
    return pl.pallas_call(
        down_kernel,
        grid=(row_total // tile,),
        in_specs=[
            pl.BlockSpec((parts, tile, units), lambda i: (0, i, 0)),
            pl.BlockSpec((full, width), lambda i: (0, 0)),
        ],
        out_specs=pl.BlockSpec((tile_blocks, PAD, width), lambda i: (i, 0, 0)),
        out_shape=jax.ShapeDtypeStruct((blocks_total, PAD, width), jnp.bfloat16),
        name="down",
    )(hidden, down_weight)


def combine_kernel(returned_ref, cols_ref, mixed_ref, sums_ref):
    rows, width = mixed_ref.shape
    slots = returned_ref.shape[0]
    cols = cols_ref[...]
    targets = cols[:, 0:2].astype(jnp.int32)
    slot_index = lax.broadcasted_iota(jnp.int32, (rows, slots), 1)
    returned = returned_ref[...]
    mixed = jnp.zeros((rows, width), jnp.float32)
    for k in range(2):
        chosen = jnp.where(slot_index == targets[:, k : k + 1], 1.0, 0.0).astype(jnp.bfloat16)
        picked = jnp.dot(chosen, returned, preferred_element_type=jnp.float32)
        mixed = mixed + picked * cols[:, 2 + k : 3 + k]
    mixed_ref[...] = mixed
    sums = jnp.sum(mixed * mixed, axis=1, keepdims=True)
    line = jnp.transpose(jnp.broadcast_to(sums, (rows, 128)))[0:1, :]
    for j in range(sums_ref.shape[0]):
        sums_ref[j] = line


def combine(returned, cols, peers):
    width = returned.shape[1]
    rows = cols.shape[0]
    return pl.pallas_call(
        combine_kernel,
        out_shape=(
            jax.ShapeDtypeStruct((rows, width), jnp.float32),
            jax.ShapeDtypeStruct((peers, 1, rows), jnp.float32),
        ),
        name="combine",
    )(returned, cols)


def final_kernel(mixed_ref, sums_ref, gain_ref, out_ref):
    rows, width = mixed_ref.shape
    peers = sums_ref.shape[0]
    total = sums_ref[0]
    for j in range(1, peers):
        total = total + sums_ref[j]
    scale = lax.rsqrt(total / (peers * width) + epsilon)
    column = jnp.transpose(jnp.broadcast_to(scale, (8, rows)))[:, 0:1]
    out_ref[...] = (mixed_ref[...] * column * gain_ref[...]).astype(jnp.bfloat16)


def final(mixed, sums, gain):
    return pl.pallas_call(
        final_kernel,
        out_shape=jax.ShapeDtypeStruct(mixed.shape, jnp.bfloat16),
        name="final",
    )(mixed, sums, gain)


def gain_rows(gain):
    first = lax.reduce_precision(gain, 8, 7)
    second = lax.reduce_precision(gain - first, 8, 7)
    third = gain - first - second
    rows = jnp.stack([first, second, third])
    return jnp.pad(rows, ((0, EXTRA - 3), (0, 0))).astype(jnp.bfloat16)


def on_device(
    tokens, expert_ids, route_weights, pre_gain, post_gain, gate_weight, up_weight, down_weight
):
    tok_rows, width = tokens.shape
    ep_count = lax.axis_size("ep")
    tp_count = lax.axis_size("tp")
    top_count = expert_ids.shape[1]
    capacity = max(2, tok_rows * top_count * 5 // (4 * ep_count))
    row_total = ep_count * capacity
    outgoing, cols = dispatch(
        tokens, jnp.transpose(expert_ids), jnp.transpose(route_weights), ep_count * PAD
    )
    arrived = lax.all_to_all(
        outgoing.reshape(ep_count, PAD, width), "ep", split_axis=0, concat_axis=0, tiled=True
    )
    arrived = arrived[:, :capacity, :].reshape(row_total, width)
    arrived = jnp.concatenate([arrived, gain_rows(pre_gain)], axis=0)
    features = lax.all_gather(arrived, "tp", axis=0, tiled=False)
    hidden = hidden_of(features, gate_weight[0], up_weight[0], row_total, 160)
    hidden_whole = lax.all_gather(hidden, "tp", axis=0, tiled=False)
    expert_out = down_of(hidden_whole, down_weight[0], ep_count, 16)
    returned = lax.all_to_all(expert_out, "ep", split_axis=0, concat_axis=0, tiled=True)
    mixed, sums = combine(returned.reshape(ep_count * PAD, width), cols, tp_count)
    sums = lax.all_to_all(sums, "tp", split_axis=0, concat_axis=0, tiled=True)
    return final(mixed, sums, post_gain[None, :])


def solution(mesh):
    return jax.shard_map(
        on_device,
        mesh=mesh,
        in_specs=(
            P("ep", "tp"),
            P("ep", None),
            P("ep", None),
            P("tp"),
            P("tp"),
            P("ep", None, "tp"),
            P("ep", None, "tp"),
            P("ep", None, "tp"),
        ),
        out_specs=P("ep", "tp"),
        check_vma=False,
    )
```

```python
import jax
import jax.numpy as jnp
from jax import lax
from jax.experimental import pallas as pl
from jax.experimental.pallas import tpu as pltpu
from jax.sharding import PartitionSpec as P

epsilon = 1e-06
PAD = 16
EXTRA = 16
FIRST = 224


def params(mebibytes):
    return pltpu.CompilerParams(vmem_limit_bytes=mebibytes << 20)


def dispatch_kernel(tok_ref, ids_ref, weights_ref, out_ref, cols_ref):
    rows = tok_ref.shape[0]
    slots = out_ref.shape[0]
    experts = slots // PAD
    ids = ids_ref[...]
    expert_index = lax.broadcasted_iota(jnp.int32, (experts, rows), 0)
    hot0 = jnp.where(expert_index == ids[0:1, :], 1.0, 0.0)
    hot1 = jnp.where(expert_index == ids[1:2, :], 1.0, 0.0)
    earlier = lax.broadcasted_iota(jnp.int32, (rows, rows), 0) < lax.broadcasted_iota(
        jnp.int32, (rows, rows), 1
    )
    earlier = jnp.where(earlier, 1.0, 0.0).astype(jnp.bfloat16)
    counts = jnp.dot((hot0 + hot1).astype(jnp.bfloat16), earlier, preferred_element_type=jnp.float32)
    slot0 = jnp.sum(hot0 * counts, axis=0, keepdims=True)
    slot1 = jnp.sum(hot1 * counts, axis=0, keepdims=True)
    target0 = ids[0:1, :] * PAD + slot0.astype(jnp.int32)
    target1 = ids[1:2, :] * PAD + slot1.astype(jnp.int32)
    slot_index = lax.broadcasted_iota(jnp.int32, (slots, rows), 0)
    chosen = jnp.logical_or(slot_index == target0, slot_index == target1)
    chosen = jnp.where(chosen, 1.0, 0.0).astype(jnp.bfloat16)
    out_ref[...] = jnp.dot(chosen, tok_ref[...], preferred_element_type=jnp.float32).astype(
        jnp.bfloat16
    )
    weights = weights_ref[...]
    lines = jnp.concatenate(
        [
            target0.astype(jnp.float32),
            target1.astype(jnp.float32),
            weights,
            jnp.zeros((4, rows), jnp.float32),
        ],
        axis=0,
    )
    cols_ref[...] = jnp.transpose(lines)


def dispatch(tokens, ids, weights, slots):
    rows, width = tokens.shape
    return pl.pallas_call(
        dispatch_kernel,
        out_shape=(
            jax.ShapeDtypeStruct((slots, width), jnp.bfloat16),
            jax.ShapeDtypeStruct((rows, 8), jnp.float32),
        ),
        compiler_params=params(8),
        name="dispatch",
    )(tokens, ids, weights)


GROUP = 16


def packed_place(shape, slot_axis, capacity):
    padded = lax.broadcasted_iota(jnp.int32, shape, slot_axis)
    packed = lax.broadcasted_iota(jnp.int32, shape, 1 - slot_axis)
    block = padded // PAD
    slot = padded - block * PAD
    same = jnp.logical_and(slot < capacity, packed == block * capacity + slot)
    return jnp.where(same, 1.0, 0.0).astype(jnp.bfloat16)


def arrange_kernel(arrived_ref, gain_ref, first_ref, second_ref):
    total = first_ref.shape[0] - EXTRA + second_ref.shape[0]
    blocks = arrived_ref.shape[0] // PAD
    capacity = total // blocks
    step = GROUP * capacity
    place = packed_place((step, GROUP * PAD), 1, capacity)
    for g in range(blocks // GROUP):
        rows = jnp.dot(
            place,
            arrived_ref[g * GROUP * PAD : (g + 1) * GROUP * PAD, :],
            preferred_element_type=jnp.float32,
        ).astype(jnp.bfloat16)
        begin = g * step
        cut = min(max(FIRST - begin, 0), step)
        if cut > 0:
            first_ref[begin : begin + cut, :] = rows[:cut, :]
        if cut < step:
            second_ref[begin + cut - FIRST : begin + step - FIRST, :] = rows[cut:, :]
    gain = gain_ref[...]
    piece0 = gain.astype(jnp.bfloat16)
    rest = gain - piece0.astype(jnp.float32)
    piece1 = rest.astype(jnp.bfloat16)
    rest = rest - piece1.astype(jnp.float32)
    piece2 = rest.astype(jnp.bfloat16)
    empty = jnp.zeros((EXTRA - 3, gain.shape[1]), jnp.float32)
    lines = jnp.concatenate(
        [
            piece0.astype(jnp.float32),
            piece1.astype(jnp.float32),
            piece2.astype(jnp.float32),
            empty,
        ],
        axis=0,
    )
    first_ref[FIRST : FIRST + EXTRA, :] = lines.astype(jnp.bfloat16)


def arrange(arrived, gain, row_total):
    width = arrived.shape[1]
    return pl.pallas_call(
        arrange_kernel,
        out_shape=(
            jax.ShapeDtypeStruct((FIRST + EXTRA, width), jnp.bfloat16),
            jax.ShapeDtypeStruct((row_total - FIRST, width), jnp.bfloat16),
        ),
        compiler_params=params(8),
        name="arrange",
    )(arrived, gain)


def hidden_rows(feat_ref, gain_ref, gate_ref, up_ref, normed_ref, rows):
    parts, _, width = feat_ref.shape
    full = parts * width
    total = jnp.zeros((rows, width), jnp.float32)
    for j in range(parts):
        part = feat_ref[j, 0:rows, :].astype(jnp.float32)
        total = total + part * part
    scale = lax.rsqrt(jnp.sum(total, axis=1, keepdims=True) / full + epsilon)
    for j in range(parts):
        pieces = gain_ref[j].astype(jnp.float32)
        gain = pieces[0:1, :] + pieces[1:2, :] + pieces[2:3, :]
        part = feat_ref[j, 0:rows, :].astype(jnp.float32)
        normed_ref[:, j * width : (j + 1) * width] = (part * scale * gain).astype(jnp.bfloat16)
    normed = normed_ref[...]
    gate = jnp.dot(normed, gate_ref[...], preferred_element_type=jnp.float32)
    upper = jnp.dot(normed, up_ref[...], preferred_element_type=jnp.float32)
    return (gate / (1.0 + jnp.exp(-gate)) * upper).astype(jnp.bfloat16)


def hidden_first_kernel(feat_ref, gain_ref, gate_ref, up_ref, out_ref, normed_ref):
    rows = out_ref.shape[0]
    out_ref[...] = hidden_rows(feat_ref, gain_ref, gate_ref, up_ref, normed_ref, rows)


def hidden_first(features, gate_weight, up_weight):
    parts, _, width = features.shape
    full, units = gate_weight.shape
    tile = FIRST // 2
    return pl.pallas_call(
        hidden_first_kernel,
        grid=(2,),
        in_specs=[
            pl.BlockSpec((parts, tile, width), lambda i: (0, i, 0)),
            pl.BlockSpec((parts, EXTRA, width), lambda i: (0, FIRST // EXTRA, 0)),
            pl.BlockSpec((full, units), lambda i: (0, 0)),
            pl.BlockSpec((full, units), lambda i: (0, 0)),
        ],
        out_specs=pl.BlockSpec((tile, units), lambda i: (i, 0)),
        out_shape=jax.ShapeDtypeStruct((FIRST, units), jnp.bfloat16),
        scratch_shapes=[pltpu.VMEM((tile, full), jnp.bfloat16)],
        compiler_params=params(16),
        name="hidden_first",
    )(features, features, gate_weight, up_weight)


def hidden_second_kernel(
    feat_ref, gain_ref, gate_ref, up_ref, first_ref, out_ref, half0_ref, half1_ref, normed_ref
):
    rows = out_ref.shape[0]
    half = half0_ref.shape[0]
    half0_ref[...] = first_ref[0:half, :]
    half1_ref[...] = first_ref[half : 2 * half, :]
    out_ref[...] = hidden_rows(feat_ref, gain_ref, gate_ref, up_ref, normed_ref, rows)


def hidden_second(features, gains, gate_weight, up_weight, first):
    parts, row_total, width = features.shape
    full, units = gate_weight.shape
    tile = row_total // 2
    half = FIRST // 2
    return pl.pallas_call(
        hidden_second_kernel,
        grid=(2,),
        in_specs=[
            pl.BlockSpec((parts, tile, width), lambda i: (0, i, 0)),
            pl.BlockSpec((parts, EXTRA, width), lambda i: (0, FIRST // EXTRA, 0)),
            pl.BlockSpec((full, units), lambda i: (0, 0)),
            pl.BlockSpec((full, units), lambda i: (0, 0)),
            pl.BlockSpec((FIRST, units), lambda i: (0, 0)),
        ],
        out_specs=(
            pl.BlockSpec((tile, units), lambda i: (i, 0)),
            pl.BlockSpec((half, units), lambda i: (0, 0)),
            pl.BlockSpec((half, units), lambda i: (0, 0)),
        ),
        out_shape=(
            jax.ShapeDtypeStruct((row_total, units), jnp.bfloat16),
            jax.ShapeDtypeStruct((half, units), jnp.bfloat16),
            jax.ShapeDtypeStruct((half, units), jnp.bfloat16),
        ),
        scratch_shapes=[pltpu.VMEM((tile, full), jnp.bfloat16)],
        compiler_params=params(16),
        name="hidden_second",
    )(features, gains, gate_weight, up_weight, first)


def down_rows(hidden_ref, down_ref):
    parts, rows, units = hidden_ref.shape
    total = jnp.zeros((rows, down_ref.shape[1]), jnp.float32)
    for j in range(parts):
        total = total + jnp.dot(
            hidden_ref[j],
            down_ref[j * units : (j + 1) * units, :],
            preferred_element_type=jnp.float32,
        )
    return total.astype(jnp.bfloat16)


def down_first_kernel(half0_ref, half1_ref, down_ref, out_ref):
    half = half0_ref.shape[1]
    out_ref[0:half, :] = down_rows(half0_ref, down_ref)
    out_ref[half : 2 * half, :] = down_rows(half1_ref, down_ref)


def down_first(half0, half1, down_weight):
    return pl.pallas_call(
        down_first_kernel,
        out_shape=jax.ShapeDtypeStruct((FIRST, down_weight.shape[1]), jnp.bfloat16),
        compiler_params=params(16),
        name="down_first",
    )(half0, half1, down_weight)


def down_second_kernel(hidden_ref, down_ref, first_ref, out_ref, result_ref):
    rows = hidden_ref.shape[1]
    total = result_ref.shape[0]
    blocks = out_ref.shape[0] // PAD
    capacity = total // blocks
    step = GROUP * capacity
    i = pl.program_id(0)
    begin = pl.multiple_of(FIRST + i * rows, 16)
    result_ref[pl.ds(begin, rows), :] = down_rows(hidden_ref, down_ref)

    @pl.when(i == pl.num_programs(0) - 1)
    def _():
        result_ref[0:FIRST, :] = first_ref[...]
        place = packed_place((GROUP * PAD, step), 0, capacity)
        for g in range(blocks // GROUP):
            out_ref[g * GROUP * PAD : (g + 1) * GROUP * PAD, :] = jnp.dot(
                place,
                result_ref[g * step : (g + 1) * step, :],
                preferred_element_type=jnp.float32,
            ).astype(jnp.bfloat16)


def down_second(hidden, down_weight, first, blocks):
    parts, rest, units = hidden.shape
    full, width = down_weight.shape
    tile = rest // 2
    return pl.pallas_call(
        down_second_kernel,
        grid=(2,),
        in_specs=[
            pl.BlockSpec((parts, tile, units), lambda i: (0, i, 0)),
            pl.BlockSpec((full, width), lambda i: (0, 0)),
            pl.BlockSpec((FIRST, width), lambda i: (0, 0)),
        ],
        out_specs=pl.BlockSpec((blocks * PAD, width), lambda i: (0, 0)),
        out_shape=jax.ShapeDtypeStruct((blocks * PAD, width), jnp.bfloat16),
        scratch_shapes=[pltpu.VMEM((FIRST + rest, width), jnp.bfloat16)],
        compiler_params=params(16),
        name="down_second",
    )(hidden, down_weight, first)


def combine_kernel(returned_ref, cols_ref, mixed_ref, sums_ref):
    rows, width = mixed_ref.shape
    slots = returned_ref.shape[0]
    cols = cols_ref[...]
    targets = cols[:, 0:2].astype(jnp.int32)
    slot_index = lax.broadcasted_iota(jnp.int32, (rows, slots), 1)
    returned = returned_ref[...]
    mixed = jnp.zeros((rows, width), jnp.float32)
    for k in range(2):
        chosen = jnp.where(slot_index == targets[:, k : k + 1], 1.0, 0.0).astype(jnp.bfloat16)
        picked = jnp.dot(chosen, returned, preferred_element_type=jnp.float32)
        mixed = mixed + picked * cols[:, 2 + k : 3 + k]
    mixed_ref[...] = mixed
    sums = jnp.sum(mixed * mixed, axis=1, keepdims=True)
    line = jnp.transpose(jnp.broadcast_to(sums, (rows, 128)))[0:1, :]
    for j in range(sums_ref.shape[0]):
        sums_ref[j] = line


def combine(returned, cols, peers):
    width = returned.shape[1]
    rows = cols.shape[0]
    return pl.pallas_call(
        combine_kernel,
        out_shape=(
            jax.ShapeDtypeStruct((rows, width), jnp.float32),
            jax.ShapeDtypeStruct((peers, 1, rows), jnp.float32),
        ),
        compiler_params=params(8),
        name="combine",
    )(returned, cols)


def final_kernel(mixed_ref, sums_ref, gain_ref, out_ref):
    rows, width = mixed_ref.shape
    peers = sums_ref.shape[0]
    total = sums_ref[0]
    for j in range(1, peers):
        total = total + sums_ref[j]
    scale = lax.rsqrt(total / (peers * width) + epsilon)
    column = jnp.transpose(jnp.broadcast_to(scale, (8, rows)))[:, 0:1]
    out_ref[...] = (mixed_ref[...] * column * gain_ref[...]).astype(jnp.bfloat16)


def final(mixed, sums, gain):
    return pl.pallas_call(
        final_kernel,
        out_shape=jax.ShapeDtypeStruct(mixed.shape, jnp.bfloat16),
        compiler_params=params(4),
        name="final",
    )(mixed, sums, gain)


def in_hbm(value):
    return pltpu.with_memory_space_constraint(value, pltpu.HBM)


def everyones(value):
    return lax.all_gather(value, "tp", axis=0, tiled=False)


def exchange(value):
    width = value.shape[1]
    blocks = value.reshape(-1, PAD, width)
    blocks = lax.all_to_all(blocks, "ep", split_axis=0, concat_axis=0, tiled=True)
    return blocks.reshape(-1, width)


def on_device(
    tokens, expert_ids, route_weights, pre_gain, post_gain, gate_weight, up_weight, down_weight
):
    tok_rows = tokens.shape[0]
    ep_count = lax.axis_size("ep")
    tp_count = lax.axis_size("tp")
    top_count = expert_ids.shape[1]
    capacity = max(2, tok_rows * top_count * 5 // (4 * ep_count))
    row_total = ep_count * capacity
    outgoing, cols = dispatch(
        in_hbm(tokens),
        in_hbm(jnp.transpose(expert_ids)),
        in_hbm(jnp.transpose(route_weights)),
        ep_count * PAD,
    )
    arrived = exchange(outgoing)
    part0, part1 = arrange(arrived, in_hbm(pre_gain[None, :]), row_total)
    features0 = everyones(part0)
    features1 = in_hbm(everyones(part1))
    hidden0 = hidden_first(features0, gate_weight[0], up_weight[0])
    hidden1, half0, half1 = hidden_second(
        features1, features0, gate_weight[0], up_weight[0], hidden0
    )
    whole1 = in_hbm(everyones(hidden1))
    result0 = down_first(everyones(half0), everyones(half1), down_weight[0])
    expert_out = down_second(whole1, down_weight[0], result0, ep_count)
    returned = exchange(expert_out)
    mixed, sums = combine(returned, cols, tp_count)
    sums = lax.all_to_all(sums, "tp", split_axis=0, concat_axis=0, tiled=True)
    return final(mixed, sums, in_hbm(post_gain[None, :]))


def solution(mesh):
    return jax.shard_map(
        on_device,
        mesh=mesh,
        in_specs=(
            P("ep", "tp"),
            P("ep", None),
            P("ep", None),
            P("tp"),
            P("tp"),
            P("ep", None, "tp"),
            P("ep", None, "tp"),
            P("ep", None, "tp"),
        ),
        out_specs=P("ep", "tp"),
        check_vma=False,
    )
```

```python
import jax
import jax.numpy as jnp
from jax import lax
from jax.experimental import pallas as pl
from jax.experimental.pallas import tpu as pltpu
from jax.sharding import Mesh, PartitionSpec as P

epsilon = 1e-06
CORES = 2
PAD = 8
EXTRA = 16
GROUP = 16
TAKEN = 120
GATHERED = 3


def params(mebibytes):
    return pltpu.CompilerParams(vmem_limit_bytes=mebibytes << 20)


def in_hbm(value):
    return pltpu.with_memory_space_constraint(value, pltpu.HBM)


def whole(memory_space=pltpu.VMEM):
    return pl.BlockSpec(memory_space=memory_space)


def prepare_kernel(tok_ref, gain_ref, out_ref):
    rows = tok_ref.shape[0]
    out_ref[0:rows, :] = tok_ref[...]
    gain = gain_ref[...]
    piece0 = gain.astype(jnp.bfloat16).astype(jnp.float32)
    piece1 = (gain - piece0).astype(jnp.bfloat16).astype(jnp.float32)
    piece2 = gain - piece0 - piece1
    empty = jnp.zeros((EXTRA - 3, gain.shape[1]), jnp.float32)
    lines = jnp.concatenate([piece0, piece1, piece2, empty], axis=0)
    out_ref[rows : rows + EXTRA, :] = lines.astype(jnp.bfloat16)


def prepare(tokens, gain):
    rows, width = tokens.shape
    return pl.pallas_call(
        prepare_kernel,
        out_shape=jax.ShapeDtypeStruct((rows + EXTRA, width), jnp.bfloat16),
        compiler_params=params(4),
        name="prepare",
    )(tokens, gain)


def dispatch_kernel(core_ref, tok_ref, ids_ref, weights_ref, out_ref, cols_ref, *, capacity):
    rows = ids_ref.shape[1]
    slots = out_ref.shape[0]
    experts = slots // PAD
    ids = ids_ref[...]
    expert_index = lax.broadcasted_iota(jnp.int32, (experts, rows), 0)
    hot0 = jnp.where(expert_index == ids[0:1, :], 1.0, 0.0)
    hot1 = jnp.where(expert_index == ids[1:2, :], 1.0, 0.0)
    earlier = lax.broadcasted_iota(jnp.int32, (rows, rows), 0) < lax.broadcasted_iota(
        jnp.int32, (rows, rows), 1
    )
    earlier = jnp.where(earlier, 1.0, 0.0).astype(jnp.bfloat16)
    counts = jnp.dot((hot0 + hot1).astype(jnp.bfloat16), earlier, preferred_element_type=jnp.float32)
    half = capacity // CORES
    targets = []
    for k, hot in enumerate((hot0, hot1)):
        slot = jnp.sum(hot * counts, axis=0, keepdims=True).astype(jnp.int32)
        slot = slot - core_ref[0] * half
        mine = jnp.logical_and(slot >= 0, slot < half)
        targets.append(jnp.where(mine, ids[k : k + 1, :] * PAD + slot, -1))
    slot_index = lax.broadcasted_iota(jnp.int32, (slots, rows), 0)
    chosen = jnp.logical_or(slot_index == targets[0], slot_index == targets[1])
    chosen = jnp.where(chosen, 1.0, 0.0).astype(jnp.bfloat16)
    width = tok_ref.shape[2]
    for c in range(CORES):
        out_ref[:, c * width : (c + 1) * width] = jnp.dot(
            chosen, tok_ref[c, 0:rows, :], preferred_element_type=jnp.float32
        ).astype(jnp.bfloat16)
    lines = jnp.concatenate(
        [
            targets[0].astype(jnp.float32),
            targets[1].astype(jnp.float32),
            weights_ref[...],
            jnp.zeros((4, rows), jnp.float32),
        ],
        axis=0,
    )
    cols_ref[...] = jnp.transpose(lines)


def dispatch(core, tokens, ids, weights, experts, capacity):
    rows = ids.shape[1]
    width = tokens.shape[2]

    def body(*refs):
        dispatch_kernel(*refs, capacity=capacity)

    return pl.pallas_call(
        body,
        in_specs=[whole(pltpu.SMEM), whole(), whole(), whole()],
        out_shape=(
            jax.ShapeDtypeStruct((experts * PAD, CORES * width), jnp.bfloat16),
            jax.ShapeDtypeStruct((rows, 8), jnp.float32),
        ),
        compiler_params=params(8),
        name="dispatch",
    )(core, tokens, ids, weights)


def packed_place(shape, slot_axis, capacity):
    padded = lax.broadcasted_iota(jnp.int32, shape, slot_axis)
    packed = lax.broadcasted_iota(jnp.int32, shape, 1 - slot_axis)
    block = padded // PAD
    slot = padded - block * PAD
    same = jnp.logical_and(slot < capacity, packed == block * capacity + slot)
    return jnp.where(same, 1.0, 0.0).astype(jnp.bfloat16)


def arrange_kernel(arrived_ref, tok_ref, first_ref, second_ref, *, half):
    step = GROUP * half
    width = tok_ref.shape[2]
    first = tok_ref.shape[1] - EXTRA
    place = packed_place((step, GROUP * PAD), 1, half)
    groups = arrived_ref.shape[0] // (GROUP * PAD)
    for g in range(groups):
        rows = jnp.dot(
            place,
            arrived_ref[g * GROUP * PAD : (g + 1) * GROUP * PAD, :],
            preferred_element_type=jnp.float32,
        ).astype(jnp.bfloat16)
        if g < GATHERED:
            first_ref[g * step : (g + 1) * step, :] = rows
        else:
            begin = (g - GATHERED) * step
            for j in range(second_ref.shape[0]):
                second_ref[j, begin : begin + step, :] = rows
    last = (groups - GATHERED) * step
    for j in range(second_ref.shape[0]):
        for c in range(CORES):
            second_ref[j, last : last + EXTRA, c * width : (c + 1) * width] = tok_ref[
                c, first : first + EXTRA, :
            ]


def arrange(arrived, tokens, chips, half):
    groups = arrived.shape[0] // (GROUP * PAD)
    width = arrived.shape[1]
    step = GROUP * half

    def body(*refs):
        arrange_kernel(*refs, half=half)

    return pl.pallas_call(
        body,
        out_shape=(
            jax.ShapeDtypeStruct((GATHERED * step, width), jnp.bfloat16),
            jax.ShapeDtypeStruct(
                (chips, (groups - GATHERED) * step + EXTRA, width), jnp.bfloat16
            ),
        ),
        compiler_params=params(8),
        name="arrange",
    )(arrived, tokens)


def hidden_kernel(
    core_ref,
    first_ref,
    second_ref,
    gate0_ref,
    up0_ref,
    gate1_ref,
    up1_ref,
    out0_ref,
    out1_ref,
    normed_ref,
    hidden_ref,
):
    chips, _, wide = first_ref.shape
    full = chips * wide
    units = gate0_ref.shape[1]
    first = first_ref.shape[1]
    last = second_ref.shape[1] - EXTRA
    for at, ref, rows in ((0, first_ref, first), (first, second_ref, last)):
        total = jnp.zeros((rows, wide), jnp.float32)
        for j in range(chips):
            part = ref[j, 0:rows, :].astype(jnp.float32)
            total = total + part * part
        scale = lax.rsqrt(jnp.sum(total, axis=1, keepdims=True) / full + epsilon)
        for j in range(chips):
            pieces = second_ref[j, last : last + EXTRA, :].astype(jnp.float32)
            gain = pieces[0:1, :] + pieces[1:2, :] + pieces[2:3, :]
            part = ref[j, 0:rows, :].astype(jnp.float32)
            normed_ref[at : at + rows, j * wide : (j + 1) * wide] = (part * scale * gain).astype(
                jnp.bfloat16
            )

    def hidden_of(gate_ref, up_ref):
        normed = normed_ref[...]
        gate = jnp.dot(normed, gate_ref[...], preferred_element_type=jnp.float32)
        upper = jnp.dot(normed, up_ref[...], preferred_element_type=jnp.float32)
        return (gate / (1.0 + jnp.exp(-gate)) * upper).astype(jnp.bfloat16)

    own = hidden_of(gate0_ref, up0_ref)
    other = hidden_of(gate1_ref, up1_ref)
    for c in range(CORES):

        @pl.when(core_ref[0] == c)
        def _():
            hidden_ref[:, c * units : (c + 1) * units] = own
            hidden_ref[:, (1 - c) * units : (2 - c) * units] = other

    rows0 = out0_ref.shape[0]
    out0_ref[...] = hidden_ref[0:rows0, :]
    for j in range(chips):
        out1_ref[j] = hidden_ref[rows0:, :]


def hidden_of(core, first, second, gate0, up0, gate1, up1):
    chips, _, wide = first.shape
    rows = first.shape[1] + second.shape[1] - EXTRA
    units = gate0.shape[1]
    return pl.pallas_call(
        hidden_kernel,
        in_specs=[whole(pltpu.SMEM)] + [whole()] * 6,
        out_shape=(
            jax.ShapeDtypeStruct((TAKEN, CORES * units), jnp.bfloat16),
            jax.ShapeDtypeStruct((chips, rows - TAKEN, CORES * units), jnp.bfloat16),
        ),
        scratch_shapes=[
            pltpu.VMEM((rows, chips * wide), jnp.bfloat16),
            pltpu.VMEM((rows, CORES * units), jnp.bfloat16),
        ],
        compiler_params=params(24),
        name="hidden",
    )(core, first, second, gate0, up0, gate1, up1)


def down_kernel(
    core_ref, hidden0_ref, hidden1_ref, down0_ref, down1_ref, out_ref, down_ref, result_ref, *, half
):
    chips, rows0, units = hidden0_ref.shape
    width = down0_ref.shape[1]
    for c in range(CORES):

        @pl.when(core_ref[0] == c)
        def _():
            down_ref[:, c * width : (c + 1) * width] = down0_ref[...]
            down_ref[:, (1 - c) * width : (2 - c) * width] = down1_ref[...]

    for at, ref in ((0, hidden0_ref), (rows0, hidden1_ref)):
        rows = ref.shape[1]
        total = jnp.zeros((rows, CORES * width), jnp.float32)
        for j in range(chips):
            total = total + jnp.dot(
                ref[j],
                down_ref[j * units : (j + 1) * units, :],
                preferred_element_type=jnp.float32,
            )
        result_ref[at : at + rows, :] = total.astype(jnp.bfloat16)
    step = GROUP * half
    place = packed_place((GROUP * PAD, step), 0, half)
    for g in range(out_ref.shape[0] // (GROUP * PAD)):
        out_ref[g * GROUP * PAD : (g + 1) * GROUP * PAD, :] = jnp.dot(
            place, result_ref[g * step : (g + 1) * step, :], preferred_element_type=jnp.float32
        ).astype(jnp.bfloat16)


def down_of(core, hidden0, hidden1, down0, down1, half):
    rows = hidden0.shape[1] + hidden1.shape[1]
    full, width = down0.shape

    def body(*refs):
        down_kernel(*refs, half=half)

    return pl.pallas_call(
        body,
        in_specs=[whole(pltpu.SMEM)] + [whole()] * 4,
        out_shape=jax.ShapeDtypeStruct((rows // half * PAD, CORES * width), jnp.bfloat16),
        scratch_shapes=[
            pltpu.VMEM((full, CORES * width), jnp.bfloat16),
            pltpu.VMEM((rows, CORES * width), jnp.bfloat16),
        ],
        compiler_params=params(24),
        name="down",
    )(core, hidden0, hidden1, down0, down1)


def combine_kernel(returned_ref, cols_ref, mixed_ref):
    _, rows, width = mixed_ref.shape
    slots = returned_ref.shape[0]
    cols = cols_ref[...]
    targets = cols[:, 0:2].astype(jnp.int32)
    slot_index = lax.broadcasted_iota(jnp.int32, (rows, slots), 1)
    returned = returned_ref[...]
    mixed = jnp.zeros((rows, CORES * width), jnp.float32)
    for k in range(2):
        chosen = jnp.where(slot_index == targets[:, k : k + 1], 1.0, 0.0).astype(jnp.bfloat16)
        picked = jnp.dot(chosen, returned, preferred_element_type=jnp.float32)
        mixed = mixed + picked * cols[:, 2 + k : 3 + k]
    for c in range(CORES):
        mixed_ref[c] = mixed[:, c * width : (c + 1) * width]


def combine(returned, cols):
    wide = returned.shape[1]
    rows = cols.shape[0]
    return pl.pallas_call(
        combine_kernel,
        out_shape=jax.ShapeDtypeStruct((CORES, rows, wide // CORES), jnp.float32),
        compiler_params=params(8),
        name="combine",
    )(returned, cols)


def sums_kernel(mixed_ref, sums_ref):
    _, rows, _ = mixed_ref.shape
    mixed = mixed_ref[0] + mixed_ref[1]
    sums = jnp.sum(mixed * mixed, axis=1, keepdims=True)
    line = jnp.transpose(jnp.broadcast_to(sums, (rows, 128)))[0:1, :]
    for j in range(sums_ref.shape[0]):
        sums_ref[j] = line


def sums_of(mixed, peers):
    return pl.pallas_call(
        sums_kernel,
        out_shape=jax.ShapeDtypeStruct((peers, 1, mixed.shape[1]), jnp.float32),
        compiler_params=params(4),
        name="sums",
    )(mixed)


def final_kernel(mixed_ref, sums_ref, gain_ref, out_ref):
    rows, width = out_ref.shape
    peers = sums_ref.shape[0]
    total = sums_ref[0]
    for j in range(1, peers):
        total = total + sums_ref[j]
    scale = lax.rsqrt(total / (peers * width) + epsilon)
    column = jnp.transpose(jnp.broadcast_to(scale, (8, rows)))[:, 0:1]
    mixed = mixed_ref[0] + mixed_ref[1]
    out_ref[...] = (mixed * column * gain_ref[...]).astype(jnp.bfloat16)


def final(mixed, sums, gain):
    return pl.pallas_call(
        final_kernel,
        out_shape=jax.ShapeDtypeStruct(mixed.shape[1:], jnp.bfloat16),
        compiler_params=params(4),
        name="final",
    )(mixed, sums, gain)


def exchange(value, axis):
    return lax.all_to_all(value, axis, split_axis=0, concat_axis=0, tiled=True)


def blocks_exchange(value):
    wide = value.shape[1]
    return exchange(value.reshape(-1, PAD, wide), "ep").reshape(-1, wide)


def swap(value):
    return lax.ppermute(value, "c", [(0, 1), (1, 0)])


def on_device(
    tokens, expert_ids, route_weights, pre_gain, post_gain, gate_weight, up_weight, down_weight
):
    tok_rows = tokens.shape[0]
    ep_count = lax.axis_size("ep")
    chips = lax.axis_size("x")
    top_count = expert_ids.shape[1]
    capacity = max(2, tok_rows * top_count * 5 // (4 * ep_count))
    half = capacity // CORES
    core = lax.axis_index("c").astype(jnp.int32).reshape(1)
    gate0, up0 = gate_weight[0], up_weight[0]
    down0 = down_weight[0]
    gate1, up1, down1 = in_hbm(swap(gate0)), in_hbm(swap(up0)), in_hbm(swap(down0))
    both = lax.all_gather(prepare(in_hbm(tokens), in_hbm(pre_gain[None, :])), "c", axis=0)
    outgoing, cols = dispatch(
        core,
        both,
        in_hbm(jnp.transpose(expert_ids)),
        in_hbm(jnp.transpose(route_weights)),
        ep_count,
        capacity,
    )
    arrived = blocks_exchange(outgoing)
    first, second = arrange(arrived, both, chips, half)
    second = exchange(second, "x")
    first = lax.all_gather(first, "x", axis=0)
    hidden0, hidden1 = hidden_of(core, first, second, gate0, up0, gate1, up1)
    hidden1 = exchange(hidden1, "x")
    hidden0 = lax.all_gather(hidden0, "x", axis=0)
    returned = blocks_exchange(down_of(core, hidden0, hidden1, down0, down1, half))
    mixed = exchange(combine(returned, cols), "c")
    sums = exchange(sums_of(mixed, chips * CORES), ("x", "c"))
    return final(mixed, sums, in_hbm(post_gain[None, :]))


def solution(mesh):
    ep_count, tp_count = mesh.devices.shape
    devices = mesh.devices.reshape(ep_count, tp_count // CORES, CORES)
    return jax.shard_map(
        on_device,
        mesh=Mesh(devices, ("ep", "x", "c")),
        in_specs=(
            P("ep", ("x", "c")),
            P("ep", None),
            P("ep", None),
            P(("x", "c")),
            P(("x", "c")),
            P("ep", None, ("x", "c")),
            P("ep", None, ("x", "c")),
            P("ep", None, ("x", "c")),
        ),
        out_specs=P("ep", ("x", "c")),
        check_vma=False,
    )
```

```python
import jax
import jax.numpy as jnp
from jax import lax
from jax.experimental import pallas as pl
from jax.experimental.pallas import tpu as pltpu
from jax.sharding import Mesh, PartitionSpec as P

epsilon = 1e-06
CORES = 2
PAD = 8
EXTRA = 16
GROUP = 16
TAKEN = 120
GATHERED = 3


def params(mebibytes):
    return pltpu.CompilerParams(vmem_limit_bytes=mebibytes << 20)


def in_hbm(value):
    return pltpu.with_memory_space_constraint(value, pltpu.HBM)


def whole(memory_space=pltpu.VMEM):
    return pl.BlockSpec(memory_space=memory_space)


def blocked(shape):
    return pl.BlockSpec(shape, lambda: (0,) * len(shape))


def dispatch_kernel(core_ref, tok_ref, ids_ref, weights_ref, out_ref, cols_ref, *, capacity):
    rows = ids_ref.shape[1]
    slots = out_ref.shape[0]
    experts = slots // PAD
    ids = ids_ref[...]
    expert_index = lax.broadcasted_iota(jnp.int32, (experts, rows), 0)
    hot0 = jnp.where(expert_index == ids[0:1, :], 1.0, 0.0)
    hot1 = jnp.where(expert_index == ids[1:2, :], 1.0, 0.0)
    earlier = lax.broadcasted_iota(jnp.int32, (rows, rows), 0) < lax.broadcasted_iota(
        jnp.int32, (rows, rows), 1
    )
    earlier = jnp.where(earlier, 1.0, 0.0).astype(jnp.bfloat16)
    counts = jnp.dot((hot0 + hot1).astype(jnp.bfloat16), earlier, preferred_element_type=jnp.float32)
    half = capacity // CORES
    targets = []
    for k, hot in enumerate((hot0, hot1)):
        slot = jnp.sum(hot * counts, axis=0, keepdims=True).astype(jnp.int32)
        slot = slot - core_ref[0] * half
        mine = jnp.logical_and(slot >= 0, slot < half)
        targets.append(jnp.where(mine, ids[k : k + 1, :] * PAD + slot, -1))
    slot_index = lax.broadcasted_iota(jnp.int32, (slots, rows), 0)
    chosen = jnp.logical_or(slot_index == targets[0], slot_index == targets[1])
    chosen = jnp.where(chosen, 1.0, 0.0).astype(jnp.bfloat16)
    width = tok_ref.shape[2]
    for c in range(CORES):
        out_ref[:, c * width : (c + 1) * width] = jnp.dot(
            chosen, tok_ref[c], preferred_element_type=jnp.float32
        ).astype(jnp.bfloat16)
    lines = jnp.concatenate(
        [
            targets[0].astype(jnp.float32),
            targets[1].astype(jnp.float32),
            weights_ref[...],
            jnp.zeros((4, rows), jnp.float32),
        ],
        axis=0,
    )
    cols_ref[...] = jnp.transpose(lines)


def dispatch(core, tokens, ids, weights, experts, capacity):
    rows = ids.shape[1]
    width = tokens.shape[2]

    def body(*refs):
        dispatch_kernel(*refs, capacity=capacity)

    return pl.pallas_call(
        body,
        in_specs=[whole(pltpu.SMEM), whole(), whole(), whole()],
        out_specs=(blocked((experts * PAD, CORES * width)), blocked((rows, 8))),
        out_shape=(
            pltpu.HBM((experts * PAD, CORES * width), jnp.bfloat16),
            pltpu.HBM((rows, 8), jnp.float32),
        ),
        compiler_params=params(8),
        name="dispatch",
    )(core, tokens, ids, weights)


def packed_place(shape, slot_axis, capacity):
    padded = lax.broadcasted_iota(jnp.int32, shape, slot_axis)
    packed = lax.broadcasted_iota(jnp.int32, shape, 1 - slot_axis)
    block = padded // PAD
    slot = padded - block * PAD
    same = jnp.logical_and(slot < capacity, packed == block * capacity + slot)
    return jnp.where(same, 1.0, 0.0).astype(jnp.bfloat16)


def pieces_of(gain):
    piece0 = gain.astype(jnp.bfloat16).astype(jnp.float32)
    piece1 = (gain - piece0).astype(jnp.bfloat16).astype(jnp.float32)
    piece2 = gain - piece0 - piece1
    empty = jnp.zeros((EXTRA - 3, gain.shape[1]), jnp.float32)
    return jnp.concatenate([piece0, piece1, piece2, empty], axis=0).astype(jnp.bfloat16)


def arrange_kernel(core_ref, arrived_ref, gain0_ref, gain1_ref, first_ref, second_ref, *, half):
    step = GROUP * half
    width = gain0_ref.shape[1]
    place = packed_place((step, GROUP * PAD), 1, half)
    groups = arrived_ref.shape[0] // (GROUP * PAD)
    for g in range(groups):
        rows = jnp.dot(
            place,
            arrived_ref[g * GROUP * PAD : (g + 1) * GROUP * PAD, :],
            preferred_element_type=jnp.float32,
        ).astype(jnp.bfloat16)
        if g < GATHERED:
            first_ref[g * step : (g + 1) * step, :] = rows
        else:
            begin = (g - GATHERED) * step
            for j in range(second_ref.shape[0]):
                second_ref[j, begin : begin + step, :] = rows
    last = (groups - GATHERED) * step
    own = pieces_of(gain0_ref[...])
    other = pieces_of(gain1_ref[...])
    for c in range(CORES):

        @pl.when(core_ref[0] == c)
        def _():
            for j in range(second_ref.shape[0]):
                second_ref[j, last : last + EXTRA, c * width : (c + 1) * width] = own
                second_ref[j, last : last + EXTRA, (1 - c) * width : (2 - c) * width] = other


def arrange(core, arrived, gain0, gain1, chips, half):
    groups = arrived.shape[0] // (GROUP * PAD)
    width = arrived.shape[1]
    step = GROUP * half
    first = (GATHERED * step, width)
    second = (chips, (groups - GATHERED) * step + EXTRA, width)

    def body(*refs):
        arrange_kernel(*refs, half=half)

    return pl.pallas_call(
        body,
        in_specs=[whole(pltpu.SMEM), whole(), whole(), whole()],
        out_specs=(blocked(first), blocked(second)),
        out_shape=(pltpu.HBM(first, jnp.bfloat16), pltpu.HBM(second, jnp.bfloat16)),
        compiler_params=params(8),
        name="arrange",
    )(core, arrived, gain0, gain1)


def hidden_kernel(
    core_ref,
    first_ref,
    second_ref,
    gate0_ref,
    up0_ref,
    gate1_ref,
    up1_ref,
    out0_ref,
    out1_ref,
    out2_ref,
    normed_ref,
    hidden_ref,
):
    chips, _, wide = first_ref.shape
    full = chips * wide
    units = gate0_ref.shape[1]
    first = first_ref.shape[1]
    last = second_ref.shape[1] - EXTRA
    for at, ref, rows in ((0, first_ref, first), (first, second_ref, last)):
        total = jnp.zeros((rows, wide), jnp.float32)
        for j in range(chips):
            part = ref[j, 0:rows, :].astype(jnp.float32)
            total = total + part * part
        scale = lax.rsqrt(jnp.sum(total, axis=1, keepdims=True) / full + epsilon)
        for j in range(chips):
            pieces = second_ref[j, last : last + EXTRA, :].astype(jnp.float32)
            gain = pieces[0:1, :] + pieces[1:2, :] + pieces[2:3, :]
            part = ref[j, 0:rows, :].astype(jnp.float32)
            normed_ref[at : at + rows, j * wide : (j + 1) * wide] = (part * scale * gain).astype(
                jnp.bfloat16
            )

    def hidden_of(gate_ref, up_ref):
        normed = normed_ref[...]
        gate = jnp.dot(normed, gate_ref[...], preferred_element_type=jnp.float32)
        upper = jnp.dot(normed, up_ref[...], preferred_element_type=jnp.float32)
        return (gate / (1.0 + jnp.exp(-gate)) * upper).astype(jnp.bfloat16)

    own = hidden_of(gate0_ref, up0_ref)
    other = hidden_of(gate1_ref, up1_ref)
    for c in range(CORES):

        @pl.when(core_ref[0] == c)
        def _():
            hidden_ref[:, c * units : (c + 1) * units] = own
            hidden_ref[:, (1 - c) * units : (2 - c) * units] = other

    rows0 = out0_ref.shape[0]
    out0_ref[...] = hidden_ref[0:rows0, :]
    out1_ref[...] = hidden_ref[rows0 : 2 * rows0, :]
    for j in range(chips):
        out2_ref[j] = hidden_ref[2 * rows0 :, :]


def hidden_of(core, first, second, gate0, up0, gate1, up1):
    chips, _, wide = first.shape
    rows = first.shape[1] + second.shape[1] - EXTRA
    units = gate0.shape[1]
    taken = (TAKEN, CORES * units)
    sent = (chips, rows - 2 * TAKEN, CORES * units)
    return pl.pallas_call(
        hidden_kernel,
        in_specs=[whole(pltpu.SMEM)] + [whole()] * 6,
        out_specs=(blocked(taken), blocked(taken), blocked(sent)),
        out_shape=(
            pltpu.HBM(taken, jnp.bfloat16),
            pltpu.HBM(taken, jnp.bfloat16),
            pltpu.HBM(sent, jnp.bfloat16),
        ),
        scratch_shapes=[
            pltpu.VMEM((rows, chips * wide), jnp.bfloat16),
            pltpu.VMEM((rows, CORES * units), jnp.bfloat16),
        ],
        compiler_params=params(24),
        name="hidden",
    )(core, first, second, gate0, up0, gate1, up1)


def down_kernel(
    core_ref,
    hidden0_ref,
    hidden1_ref,
    hidden2_ref,
    down0_ref,
    down1_ref,
    out_ref,
    down_ref,
    result_ref,
    *,
    half,
):
    chips, rows0, units = hidden0_ref.shape
    width = down0_ref.shape[1]
    for c in range(CORES):

        @pl.when(core_ref[0] == c)
        def _():
            down_ref[:, c * width : (c + 1) * width] = down0_ref[...]
            down_ref[:, (1 - c) * width : (2 - c) * width] = down1_ref[...]

    for at, ref in ((0, hidden0_ref), (rows0, hidden1_ref), (2 * rows0, hidden2_ref)):
        rows = ref.shape[1]
        total = jnp.zeros((rows, CORES * width), jnp.float32)
        for j in range(chips):
            total = total + jnp.dot(
                ref[j],
                down_ref[j * units : (j + 1) * units, :],
                preferred_element_type=jnp.float32,
            )
        result_ref[at : at + rows, :] = total.astype(jnp.bfloat16)
    step = GROUP * half
    place = packed_place((GROUP * PAD, step), 0, half)
    for g in range(out_ref.shape[0] // (GROUP * PAD)):
        out_ref[g * GROUP * PAD : (g + 1) * GROUP * PAD, :] = jnp.dot(
            place, result_ref[g * step : (g + 1) * step, :], preferred_element_type=jnp.float32
        ).astype(jnp.bfloat16)


def down_of(core, hidden0, hidden1, hidden2, down0, down1, half):
    rows = hidden0.shape[1] + hidden1.shape[1] + hidden2.shape[1]
    full, width = down0.shape

    def body(*refs):
        down_kernel(*refs, half=half)

    return pl.pallas_call(
        body,
        in_specs=[whole(pltpu.SMEM)] + [whole()] * 5,
        out_shape=jax.ShapeDtypeStruct((rows // half * PAD, CORES * width), jnp.bfloat16),
        scratch_shapes=[
            pltpu.VMEM((full, CORES * width), jnp.bfloat16),
            pltpu.VMEM((rows, CORES * width), jnp.bfloat16),
        ],
        compiler_params=params(24),
        name="down",
    )(core, hidden0, hidden1, hidden2, down0, down1)


def combine_kernel(returned_ref, cols_ref, mixed_ref):
    rows, wide = mixed_ref.shape
    slots = returned_ref.shape[0]
    cols = cols_ref[...]
    targets = cols[:, 0:2].astype(jnp.int32)
    slot_index = lax.broadcasted_iota(jnp.int32, (rows, slots), 1)
    returned = returned_ref[...]
    mixed = jnp.zeros((rows, wide), jnp.float32)
    for k in range(2):
        chosen = jnp.where(slot_index == targets[:, k : k + 1], 1.0, 0.0).astype(jnp.bfloat16)
        picked = jnp.dot(chosen, returned, preferred_element_type=jnp.float32)
        mixed = mixed + picked * cols[:, 2 + k : 3 + k]
    mixed_ref[...] = mixed


def combine(returned, cols):
    return pl.pallas_call(
        combine_kernel,
        out_shape=jax.ShapeDtypeStruct((cols.shape[0], returned.shape[1]), jnp.float32),
        compiler_params=params(8),
        name="combine",
    )(returned, cols)


def sums_kernel(core_ref, parts_ref, mixed_ref, sums_ref):
    rows, width = mixed_ref.shape
    for c in range(CORES):

        @pl.when(core_ref[0] == c)
        def _():
            own = slice(c * width, (c + 1) * width)
            mixed_ref[...] = parts_ref[0, :, own] + parts_ref[1, :, own]

    mixed = mixed_ref[...]
    sums = jnp.sum(mixed * mixed, axis=1, keepdims=True)
    line = jnp.transpose(jnp.broadcast_to(sums, (rows, 128)))[0:1, :]
    for j in range(sums_ref.shape[0]):
        sums_ref[j] = line


def sums_of(core, parts, peers):
    _, rows, wide = parts.shape
    return pl.pallas_call(
        sums_kernel,
        in_specs=[whole(pltpu.SMEM), whole()],
        out_shape=(
            jax.ShapeDtypeStruct((rows, wide // CORES), jnp.float32),
            jax.ShapeDtypeStruct((peers, 1, rows), jnp.float32),
        ),
        compiler_params=params(4),
        name="sums",
    )(core, parts)


def final_kernel(mixed_ref, sums_ref, gain_ref, out_ref):
    rows, width = mixed_ref.shape
    peers = sums_ref.shape[0]
    total = sums_ref[0]
    for j in range(1, peers):
        total = total + sums_ref[j]
    scale = lax.rsqrt(total / (peers * width) + epsilon)
    column = jnp.transpose(jnp.broadcast_to(scale, (8, rows)))[:, 0:1]
    out_ref[...] = (mixed_ref[...] * column * gain_ref[...]).astype(jnp.bfloat16)


def final(mixed, sums, gain):
    return pl.pallas_call(
        final_kernel,
        out_shape=jax.ShapeDtypeStruct(mixed.shape, jnp.bfloat16),
        compiler_params=params(4),
        name="final",
    )(mixed, sums, gain)


def exchange(value, axis):
    return lax.all_to_all(value, axis, split_axis=0, concat_axis=0, tiled=True)


def blocks_exchange(value):
    wide = value.shape[1]
    return exchange(value.reshape(-1, PAD, wide), "ep").reshape(-1, wide)


def swap(value):
    return lax.ppermute(value, "c", [(0, 1), (1, 0)])


def on_device(
    tokens, expert_ids, route_weights, pre_gain, post_gain, gate_weight, up_weight, down_weight
):
    tok_rows = tokens.shape[0]
    ep_count = lax.axis_size("ep")
    chips = lax.axis_size("x")
    top_count = expert_ids.shape[1]
    capacity = max(2, tok_rows * top_count * 5 // (4 * ep_count))
    half = capacity // CORES
    core = lax.axis_index("c").astype(jnp.int32).reshape(1)
    gate0, up0 = gate_weight[0], up_weight[0]
    down0 = down_weight[0]
    gain0 = pre_gain[None, :]
    gate1, up1, down1 = in_hbm(swap(gate0)), in_hbm(swap(up0)), swap(down0)
    gain1 = in_hbm(swap(gain0))
    outgoing, cols = dispatch(
        core,
        lax.all_gather(tokens, "c", axis=0),
        in_hbm(jnp.transpose(expert_ids)),
        in_hbm(jnp.transpose(route_weights)),
        ep_count,
        capacity,
    )
    arrived, down1 = lax.optimization_barrier((blocks_exchange(outgoing), down1))
    first, second = arrange(core, arrived, in_hbm(gain0), gain1, chips, half)
    second = exchange(second, "x")
    first = lax.all_gather(first, "x", axis=0)
    hidden0, hidden1, hidden2 = hidden_of(core, first, second, gate0, up0, gate1, up1)
    hidden2 = exchange(hidden2, "x")
    hidden0 = lax.all_gather(hidden0, "x", axis=0)
    hidden1 = lax.all_gather(hidden1, "x", axis=0)
    result = down_of(core, hidden0, hidden1, hidden2, down0, in_hbm(down1), half)
    mixed = lax.all_gather(combine(blocks_exchange(result), cols), "c", axis=0)
    mixed, sums = sums_of(core, mixed, chips * CORES)
    sums = exchange(sums, ("x", "c"))
    return final(mixed, sums, in_hbm(post_gain[None, :]))


def solution(mesh):
    ep_count, tp_count = mesh.devices.shape
    devices = mesh.devices.reshape(ep_count, tp_count // CORES, CORES)
    return jax.shard_map(
        on_device,
        mesh=Mesh(devices, ("ep", "x", "c")),
        in_specs=(
            P("ep", ("x", "c")),
            P("ep", None),
            P("ep", None),
            P(("x", "c")),
            P(("x", "c")),
            P("ep", None, ("x", "c")),
            P("ep", None, ("x", "c")),
            P("ep", None, ("x", "c")),
        ),
        out_specs=P("ep", ("x", "c")),
        check_vma=False,
    )
```

```python
import jax
import jax.numpy as jnp
from jax import lax
from jax.experimental import pallas as pl
from jax.experimental.pallas import tpu as pltpu
from jax.sharding import Mesh, PartitionSpec as P

epsilon = 1e-06
CORES = 2
PAD = 8
EXTRA = 16
GROUP = 16


def params(mebibytes):
    return pltpu.CompilerParams(vmem_limit_bytes=mebibytes << 20)


def in_hbm(value):
    return pltpu.with_memory_space_constraint(value, pltpu.HBM)


def whole(memory_space=pltpu.VMEM):
    return pl.BlockSpec(memory_space=memory_space)


def prepare_kernel(tok_ref, gain_ref, out_ref):
    rows = tok_ref.shape[0]
    out_ref[0:rows, :] = tok_ref[...]
    gain = gain_ref[...]
    piece0 = gain.astype(jnp.bfloat16).astype(jnp.float32)
    piece1 = (gain - piece0).astype(jnp.bfloat16).astype(jnp.float32)
    piece2 = gain - piece0 - piece1
    empty = jnp.zeros((EXTRA - 3, gain.shape[1]), jnp.float32)
    lines = jnp.concatenate([piece0, piece1, piece2, empty], axis=0)
    out_ref[rows : rows + EXTRA, :] = lines.astype(jnp.bfloat16)


def prepare(tokens, gain):
    rows, width = tokens.shape
    return pl.pallas_call(
        prepare_kernel,
        out_shape=jax.ShapeDtypeStruct((rows + EXTRA, width), jnp.bfloat16),
        compiler_params=params(4),
        name="prepare",
    )(tokens, gain)


def dispatch_kernel(place_ref, tok_ref, ids_ref, weights_ref, out_ref, cols_ref, *, capacity):
    rows = ids_ref.shape[1]
    slots = out_ref.shape[0]
    experts = slots // PAD
    ids = ids_ref[...]
    expert_index = lax.broadcasted_iota(jnp.int32, (experts, rows), 0)
    hot0 = jnp.where(expert_index == ids[0:1, :], 1.0, 0.0)
    hot1 = jnp.where(expert_index == ids[1:2, :], 1.0, 0.0)
    earlier = lax.broadcasted_iota(jnp.int32, (rows, rows), 0) < lax.broadcasted_iota(
        jnp.int32, (rows, rows), 1
    )
    earlier = jnp.where(earlier, 1.0, 0.0).astype(jnp.bfloat16)
    counts = jnp.dot((hot0 + hot1).astype(jnp.bfloat16), earlier, preferred_element_type=jnp.float32)
    half = capacity // CORES
    targets = []
    for k, hot in enumerate((hot0, hot1)):
        slot = jnp.sum(hot * counts, axis=0, keepdims=True).astype(jnp.int32)
        slot = slot - place_ref[1] * half
        mine = jnp.logical_and(slot >= 0, slot < half)
        targets.append(jnp.where(mine, ids[k : k + 1, :] * PAD + slot, -1))
    slot_index = lax.broadcasted_iota(jnp.int32, (slots, rows), 0)
    chosen = jnp.logical_or(slot_index == targets[0], slot_index == targets[1])
    chosen = jnp.where(chosen, 1.0, 0.0).astype(jnp.bfloat16)
    width = tok_ref.shape[2]
    for c in range(CORES):
        out_ref[:, c * width : (c + 1) * width] = jnp.dot(
            chosen, tok_ref[c, 0:rows, :], preferred_element_type=jnp.float32
        ).astype(jnp.bfloat16)
    lines = jnp.concatenate(
        [
            targets[0].astype(jnp.float32),
            targets[1].astype(jnp.float32),
            weights_ref[...],
            jnp.zeros((4, rows), jnp.float32),
        ],
        axis=0,
    )
    cols_ref[...] = jnp.transpose(lines)


def dispatch(place, tokens, ids, weights, experts, capacity):
    rows = ids.shape[1]
    width = tokens.shape[2]

    def body(*refs):
        dispatch_kernel(*refs, capacity=capacity)

    return pl.pallas_call(
        body,
        in_specs=[whole(pltpu.SMEM), whole(), whole(), whole()],
        out_shape=(
            jax.ShapeDtypeStruct((experts * PAD, CORES * width), jnp.bfloat16),
            pltpu.HBM((rows, 8), jnp.float32),
        ),
        compiler_params=params(8),
        name="dispatch",
    )(place, tokens, ids, weights)


def packed_place(shape, slot_axis, capacity):
    padded = lax.broadcasted_iota(jnp.int32, shape, slot_axis)
    packed = lax.broadcasted_iota(jnp.int32, shape, 1 - slot_axis)
    block = padded // PAD
    slot = padded - block * PAD
    same = jnp.logical_and(slot < capacity, packed == block * capacity + slot)
    return jnp.where(same, 1.0, 0.0).astype(jnp.bfloat16)


def arrange_kernel(arrived_ref, tok_ref, out_ref, *, half):
    step = GROUP * half
    width = tok_ref.shape[2]
    first = tok_ref.shape[1] - EXTRA
    chips, rows, _ = out_ref.shape
    place = packed_place((step, GROUP * PAD), 1, half)
    for g in range(arrived_ref.shape[0] // (GROUP * PAD)):
        packed = jnp.dot(
            place,
            arrived_ref[g * GROUP * PAD : (g + 1) * GROUP * PAD, :],
            preferred_element_type=jnp.float32,
        ).astype(jnp.bfloat16)
        for j in range(chips):
            out_ref[j, g * step : (g + 1) * step, :] = packed
    for j in range(chips):
        for c in range(CORES):
            out_ref[j, rows - EXTRA :, c * width : (c + 1) * width] = tok_ref[
                c, first : first + EXTRA, :
            ]


def arrange(arrived, tokens, chips, half):
    blocks = arrived.shape[0] // PAD
    width = arrived.shape[1]

    def body(*refs):
        arrange_kernel(*refs, half=half)

    return pl.pallas_call(
        body,
        out_shape=jax.ShapeDtypeStruct((chips, blocks * half + EXTRA, width), jnp.bfloat16),
        compiler_params=params(8),
        name="arrange",
    )(arrived, tokens)


def hidden_kernel(
    place_ref, feat_ref, gate0_ref, up0_ref, gate1_ref, up1_ref, out_ref, normed_ref
):
    chips, rows, wide = feat_ref.shape
    rows = rows - EXTRA
    full = chips * wide
    units = gate0_ref.shape[1]
    total = jnp.zeros((rows, wide), jnp.float32)
    for j in range(chips):
        part = feat_ref[j, 0:rows, :].astype(jnp.float32)
        total = total + part * part
    scale = lax.rsqrt(jnp.sum(total, axis=1, keepdims=True) / full + epsilon)
    for j in range(chips):
        pieces = feat_ref[j, rows : rows + EXTRA, :].astype(jnp.float32)
        gain = pieces[0:1, :] + pieces[1:2, :] + pieces[2:3, :]
        part = feat_ref[j, 0:rows, :].astype(jnp.float32)
        normed_ref[:, j * wide : (j + 1) * wide] = (part * scale * gain).astype(jnp.bfloat16)

    def hidden_of(gate_ref, up_ref):
        normed = normed_ref[...]
        gate = jnp.dot(normed, gate_ref[...], preferred_element_type=jnp.float32)
        upper = jnp.dot(normed, up_ref[...], preferred_element_type=jnp.float32)
        return (gate / (1.0 + jnp.exp(-gate)) * upper).astype(jnp.bfloat16)

    own = hidden_of(gate0_ref, up0_ref)
    other = hidden_of(gate1_ref, up1_ref)
    for c in range(CORES):

        @pl.when(place_ref[1] == c)
        def _():
            out_ref[:, c * units : (c + 1) * units] = own
            out_ref[:, (1 - c) * units : (2 - c) * units] = other


def hidden_of(place, features, gate0, up0, gate1, up1):
    chips, rows, wide = features.shape
    units = gate0.shape[1]
    return pl.pallas_call(
        hidden_kernel,
        in_specs=[whole(pltpu.SMEM)] + [whole()] * 5,
        out_shape=jax.ShapeDtypeStruct((rows - EXTRA, CORES * units), jnp.bfloat16),
        scratch_shapes=[pltpu.VMEM((rows - EXTRA, chips * wide), jnp.bfloat16)],
        compiler_params=params(24),
        name="hidden",
    )(place, features, gate0, up0, gate1, up1)


def down_kernel(*refs, offsets, half):
    place_ref, *hidden_refs, down0_ref, down1_ref, out_ref, down_ref, result_ref = refs
    rows, units = hidden_refs[0].shape
    width = down0_ref.shape[1]
    for c in range(CORES):

        @pl.when(place_ref[1] == c)
        def _():
            down_ref[:, c * width : (c + 1) * width] = down0_ref[...]
            down_ref[:, (1 - c) * width : (2 - c) * width] = down1_ref[...]

    chips = len(offsets)
    total = jnp.zeros((rows, CORES * width), jnp.float32)
    for offset, ref in zip(offsets, hidden_refs):
        chip = lax.rem(place_ref[0] + (offset + chips), chips)
        begin = pl.multiple_of(chip * units, units)
        total = total + jnp.dot(
            ref[...], down_ref[pl.ds(begin, units), :], preferred_element_type=jnp.float32
        )
    result_ref[...] = total.astype(jnp.bfloat16)
    step = GROUP * half
    place = packed_place((GROUP * PAD, step), 0, half)
    for g in range(out_ref.shape[0] // (GROUP * PAD)):
        out_ref[g * GROUP * PAD : (g + 1) * GROUP * PAD, :] = jnp.dot(
            place, result_ref[g * step : (g + 1) * step, :], preferred_element_type=jnp.float32
        ).astype(jnp.bfloat16)


def down_of(place, hiddens, down0, down1, half):
    offsets = [offset for offset, _ in hiddens]
    arrays = [array for _, array in hiddens]
    rows = arrays[0].shape[0]
    full, width = down0.shape

    def body(*refs):
        down_kernel(*refs, offsets=offsets, half=half)

    return pl.pallas_call(
        body,
        in_specs=[whole(pltpu.SMEM)] + [whole()] * (len(arrays) + 2),
        out_shape=jax.ShapeDtypeStruct((rows // half * PAD, CORES * width), jnp.bfloat16),
        scratch_shapes=[
            pltpu.VMEM((full, CORES * width), jnp.bfloat16),
            pltpu.VMEM((rows, CORES * width), jnp.bfloat16),
        ],
        compiler_params=params(24),
        name="down",
    )(place, *arrays, down0, down1)


def combine_kernel(returned_ref, cols_ref, mixed_ref):
    rows, wide = mixed_ref.shape
    slots = returned_ref.shape[0]
    cols = cols_ref[...]
    targets = cols[:, 0:2].astype(jnp.int32)
    slot_index = lax.broadcasted_iota(jnp.int32, (rows, slots), 1)
    returned = returned_ref[...]
    mixed = jnp.zeros((rows, wide), jnp.float32)
    for k in range(2):
        chosen = jnp.where(slot_index == targets[:, k : k + 1], 1.0, 0.0).astype(jnp.bfloat16)
        picked = jnp.dot(chosen, returned, preferred_element_type=jnp.float32)
        mixed = mixed + picked * cols[:, 2 + k : 3 + k]
    mixed_ref[...] = mixed


def combine(returned, cols):
    return pl.pallas_call(
        combine_kernel,
        out_shape=jax.ShapeDtypeStruct((cols.shape[0], returned.shape[1]), jnp.float32),
        compiler_params=params(8),
        name="combine",
    )(returned, cols)


def sums_kernel(place_ref, parts_ref, mixed_ref, sums_ref):
    rows, width = mixed_ref.shape
    for c in range(CORES):

        @pl.when(place_ref[1] == c)
        def _():
            own = slice(c * width, (c + 1) * width)
            mixed_ref[...] = parts_ref[0, :, own] + parts_ref[1, :, own]

    mixed = mixed_ref[...]
    sums = jnp.sum(mixed * mixed, axis=1, keepdims=True)
    line = jnp.transpose(jnp.broadcast_to(sums, (rows, 128)))[0:1, :]
    for j in range(sums_ref.shape[0]):
        sums_ref[j] = line


def sums_of(place, parts, peers):
    _, rows, wide = parts.shape
    return pl.pallas_call(
        sums_kernel,
        in_specs=[whole(pltpu.SMEM), whole()],
        out_shape=(
            jax.ShapeDtypeStruct((rows, wide // CORES), jnp.float32),
            jax.ShapeDtypeStruct((peers, 1, rows), jnp.float32),
        ),
        compiler_params=params(4),
        name="sums",
    )(place, parts)


def final_kernel(mixed_ref, sums_ref, gain_ref, out_ref):
    rows, width = mixed_ref.shape
    peers = sums_ref.shape[0]
    total = sums_ref[0]
    for j in range(1, peers):
        total = total + sums_ref[j]
    scale = lax.rsqrt(total / (peers * width) + epsilon)
    column = jnp.transpose(jnp.broadcast_to(scale, (8, rows)))[:, 0:1]
    out_ref[...] = (mixed_ref[...] * column * gain_ref[...]).astype(jnp.bfloat16)


def final(mixed, sums, gain):
    return pl.pallas_call(
        final_kernel,
        out_shape=jax.ShapeDtypeStruct(mixed.shape, jnp.bfloat16),
        compiler_params=params(4),
        name="final",
    )(mixed, sums, gain)


def exchange(value, axis):
    return lax.all_to_all(value, axis, split_axis=0, concat_axis=0, tiled=True)


def blocks_exchange(value):
    wide = value.shape[1]
    return exchange(value.reshape(-1, PAD, wide), "ep").reshape(-1, wide)


def swap(value):
    return lax.ppermute(value, "c", [(0, 1), (1, 0)])


def ring(value):
    chips = lax.axis_size("x")
    onward = [(i, (i + 1) % chips) for i in range(chips)]
    backward = [(i, (i - 1) % chips) for i in range(chips)]
    arrays = [(0, value)]
    before, after = value, value
    for step in range(1, chips // 2 + 1):
        before = lax.ppermute(before, "x", onward)
        arrays.append((-step, before))
        if step < chips - step:
            after = lax.ppermute(after, "x", backward)
            arrays.append((step, after))
    return arrays


def on_device(
    tokens, expert_ids, route_weights, pre_gain, post_gain, gate_weight, up_weight, down_weight
):
    tok_rows = tokens.shape[0]
    ep_count = lax.axis_size("ep")
    chips = lax.axis_size("x")
    top_count = expert_ids.shape[1]
    capacity = max(2, tok_rows * top_count * 5 // (4 * ep_count))
    half = capacity // CORES
    place = jnp.stack([lax.axis_index("x"), lax.axis_index("c")]).astype(jnp.int32)
    gate0, up0, down0 = gate_weight[0], up_weight[0], down_weight[0]
    gate1, up1 = in_hbm(swap(gate0)), in_hbm(swap(up0))
    both = lax.all_gather(prepare(in_hbm(tokens), in_hbm(pre_gain[None, :])), "c", axis=0)
    outgoing, cols = dispatch(
        place,
        both,
        in_hbm(jnp.transpose(expert_ids)),
        in_hbm(jnp.transpose(route_weights)),
        ep_count,
        capacity,
    )
    outgoing, later = lax.optimization_barrier((outgoing, down0))
    arrived, down1 = lax.optimization_barrier((blocks_exchange(outgoing), swap(later)))
    features = exchange(arrange(arrived, both, chips, half), "x")
    hidden = hidden_of(place, features, gate0, up0, gate1, up1)
    result = down_of(place, ring(hidden), in_hbm(down0), in_hbm(down1), half)
    mixed = lax.all_gather(combine(blocks_exchange(result), cols), "c", axis=0)
    mixed, sums = sums_of(place, mixed, chips * CORES)
    sums = exchange(sums, ("x", "c"))
    return final(mixed, sums, in_hbm(post_gain[None, :]))


def solution(mesh):
    ep_count, tp_count = mesh.devices.shape
    devices = mesh.devices.reshape(ep_count, tp_count // CORES, CORES)
    return jax.shard_map(
        on_device,
        mesh=Mesh(devices, ("ep", "x", "c")),
        in_specs=(
            P("ep", ("x", "c")),
            P("ep", None),
            P("ep", None),
            P(("x", "c")),
            P(("x", "c")),
            P("ep", None, ("x", "c")),
            P("ep", None, ("x", "c")),
            P("ep", None, ("x", "c")),
        ),
        out_specs=P("ep", ("x", "c")),
        check_vma=False,
    )
```

```python
import jax
import jax.numpy as jnp
from jax import lax
from jax.experimental import pallas as pl
from jax.experimental.pallas import tpu as pltpu
from jax.sharding import Mesh, PartitionSpec as P


epsilon = 1e-06
CORES = 2
PAD = 8
EXTRA = 16
GROUP = 16


def params(mebibytes):
    return pltpu.CompilerParams(vmem_limit_bytes=mebibytes << 20)


def in_hbm(value):
    return pltpu.with_memory_space_constraint(value, pltpu.HBM)


def whole(memory_space=pltpu.VMEM):
    return pl.BlockSpec(memory_space=memory_space)


def prepare_kernel(tok_ref, gain_ref, out_ref):
    rows = tok_ref.shape[0]
    out_ref[0:rows, :] = tok_ref[...]
    gain = gain_ref[...]
    piece0 = gain.astype(jnp.bfloat16).astype(jnp.float32)
    piece1 = (gain - piece0).astype(jnp.bfloat16).astype(jnp.float32)
    piece2 = gain - piece0 - piece1
    empty = jnp.zeros((EXTRA - 3, gain.shape[1]), jnp.float32)
    lines = jnp.concatenate([piece0, piece1, piece2, empty], axis=0)
    out_ref[rows : rows + EXTRA, :] = lines.astype(jnp.bfloat16)


def prepare(tokens, gain):
    rows, width = tokens.shape
    return pl.pallas_call(
        prepare_kernel,
        out_shape=jax.ShapeDtypeStruct((rows + EXTRA, width), jnp.bfloat16),
        compiler_params=params(4),
        name="prepare",
    )(tokens, gain)


def dispatch_kernel(place_ref, tok_ref, ids_ref, weights_ref, out_ref, cols_ref, *, capacity):
    rows = ids_ref.shape[1]
    slots = out_ref.shape[0]
    experts = slots // PAD
    ids = ids_ref[...]
    expert_index = lax.broadcasted_iota(jnp.int32, (experts, rows), 0)
    hot0 = jnp.where(expert_index == ids[0:1, :], 1.0, 0.0)
    hot1 = jnp.where(expert_index == ids[1:2, :], 1.0, 0.0)
    earlier = lax.broadcasted_iota(jnp.int32, (rows, rows), 0) < lax.broadcasted_iota(
        jnp.int32, (rows, rows), 1
    )
    earlier = jnp.where(earlier, 1.0, 0.0).astype(jnp.bfloat16)
    counts = jnp.dot((hot0 + hot1).astype(jnp.bfloat16), earlier, preferred_element_type=jnp.float32)
    half = capacity // CORES
    targets = []
    for k, hot in enumerate((hot0, hot1)):
        slot = jnp.sum(hot * counts, axis=0, keepdims=True).astype(jnp.int32)
        slot = slot - place_ref[1] * half
        mine = jnp.logical_and(slot >= 0, slot < half)
        targets.append(jnp.where(mine, ids[k : k + 1, :] * PAD + slot, -1))
    slot_index = lax.broadcasted_iota(jnp.int32, (slots, rows), 0)
    chosen = jnp.logical_or(slot_index == targets[0], slot_index == targets[1])
    chosen = jnp.where(chosen, 1.0, 0.0).astype(jnp.bfloat16)
    width = tok_ref.shape[2]
    for c in range(CORES):
        out_ref[:, c * width : (c + 1) * width] = jnp.dot(
            chosen, tok_ref[c, 0:rows, :], preferred_element_type=jnp.float32
        ).astype(jnp.bfloat16)
    lines = jnp.concatenate(
        [
            targets[0].astype(jnp.float32),
            targets[1].astype(jnp.float32),
            weights_ref[...],
            jnp.zeros((4, rows), jnp.float32),
        ],
        axis=0,
    )
    cols_ref[...] = jnp.transpose(lines)


def dispatch(place, tokens, ids, weights, experts, capacity):
    rows = ids.shape[1]
    width = tokens.shape[2]

    def body(*refs):
        dispatch_kernel(*refs, capacity=capacity)

    return pl.pallas_call(
        body,
        in_specs=[whole(pltpu.SMEM), whole(), whole(), whole()],
        out_shape=(
            jax.ShapeDtypeStruct((experts * PAD, CORES * width), jnp.bfloat16),
            pltpu.HBM((rows, 8), jnp.float32),
        ),
        compiler_params=params(8),
        name="dispatch",
    )(place, tokens, ids, weights)


def packed_place(shape, slot_axis, capacity):
    padded = lax.broadcasted_iota(jnp.int32, shape, slot_axis)
    packed = lax.broadcasted_iota(jnp.int32, shape, 1 - slot_axis)
    block = padded // PAD
    slot = padded - block * PAD
    same = jnp.logical_and(slot < capacity, packed == block * capacity + slot)
    return jnp.where(same, 1.0, 0.0).astype(jnp.bfloat16)


def arrange_kernel(arrived_ref, tok_ref, out_ref, *, half):
    step = GROUP * half
    width = tok_ref.shape[2]
    first = tok_ref.shape[1] - EXTRA
    chips, rows, _ = out_ref.shape
    place = packed_place((step, GROUP * PAD), 1, half)
    for g in range(arrived_ref.shape[0] // (GROUP * PAD)):
        packed = jnp.dot(
            place,
            arrived_ref[g * GROUP * PAD : (g + 1) * GROUP * PAD, :],
            preferred_element_type=jnp.float32,
        ).astype(jnp.bfloat16)
        for j in range(chips):
            out_ref[j, g * step : (g + 1) * step, :] = packed
    for j in range(chips):
        for c in range(CORES):
            out_ref[j, rows - EXTRA :, c * width : (c + 1) * width] = tok_ref[
                c, first : first + EXTRA, :
            ]


def arrange(arrived, tokens, chips, half):
    blocks = arrived.shape[0] // PAD
    width = arrived.shape[1]

    def body(*refs):
        arrange_kernel(*refs, half=half)

    return pl.pallas_call(
        body,
        out_shape=jax.ShapeDtypeStruct((chips, blocks * half + EXTRA, width), jnp.bfloat16),
        compiler_params=params(8),
        name="arrange",
    )(arrived, tokens)


def hidden_kernel(
    place_ref, feat_ref, gate0_ref, up0_ref, gate1_ref, up1_ref, out_ref, normed_ref
):
    chips, rows, wide = feat_ref.shape
    rows = rows - EXTRA
    full = chips * wide
    units = gate0_ref.shape[1]
    total = jnp.zeros((rows, wide), jnp.float32)
    for j in range(chips):
        part = feat_ref[j, 0:rows, :].astype(jnp.float32)
        total = total + part * part
    scale = lax.rsqrt(jnp.sum(total, axis=1, keepdims=True) / full + epsilon)
    for j in range(chips):
        pieces = feat_ref[j, rows : rows + EXTRA, :].astype(jnp.float32)
        gain = pieces[0:1, :] + pieces[1:2, :] + pieces[2:3, :]
        part = feat_ref[j, 0:rows, :].astype(jnp.float32)
        normed_ref[:, j * wide : (j + 1) * wide] = (part * scale * gain).astype(jnp.bfloat16)

    def hidden_of(gate_ref, up_ref):
        normed = normed_ref[...]
        gate = jnp.dot(normed, gate_ref[...], preferred_element_type=jnp.float32)
        upper = jnp.dot(normed, up_ref[...], preferred_element_type=jnp.float32)
        return (gate / (1.0 + jnp.exp(-gate)) * upper).astype(jnp.bfloat16)

    own = hidden_of(gate0_ref, up0_ref)
    other = hidden_of(gate1_ref, up1_ref)
    for c in range(CORES):

        @pl.when(place_ref[1] == c)
        def _():
            out_ref[:, c * units : (c + 1) * units] = own
            out_ref[:, (1 - c) * units : (2 - c) * units] = other


def hidden_of(place, features, gate0, up0, gate1, up1):
    chips, rows, wide = features.shape
    units = gate0.shape[1]
    return pl.pallas_call(
        hidden_kernel,
        in_specs=[whole(pltpu.SMEM)] + [whole()] * 5,
        out_shape=jax.ShapeDtypeStruct((rows - EXTRA, CORES * units), jnp.bfloat16),
        scratch_shapes=[pltpu.VMEM((rows - EXTRA, chips * wide), jnp.bfloat16)],
        compiler_params=params(24),
        name="hidden",
    )(place, features, gate0, up0, gate1, up1)


def both_columns(place_ref, down0_ref, down1_ref, down_ref):
    width = down0_ref.shape[1]
    for c in range(CORES):

        @pl.when(place_ref[1] == c)
        def _():
            down_ref[:, c * width : (c + 1) * width] = down0_ref[...]
            down_ref[:, (1 - c) * width : (2 - c) * width] = down1_ref[...]


def down_early_kernel(*refs, offsets, chips):
    place_ref, *hidden_refs, down0_ref, down1_ref, out_ref, down_ref = refs
    _, units = hidden_refs[0].shape
    both_columns(place_ref, down0_ref, down1_ref, down_ref)
    total = jnp.zeros(out_ref.shape, jnp.float32)
    for offset, ref in zip(offsets, hidden_refs):
        chip = lax.rem(place_ref[0] + (offset + chips), chips)
        begin = pl.multiple_of(chip * units, units)
        total = total + jnp.dot(
            ref[...], down_ref[pl.ds(begin, units), :], preferred_element_type=jnp.float32
        )
    out_ref[...] = total


def down_early(place, hiddens, down0, down1, chips):
    offsets = [offset for offset, _ in hiddens]
    arrays = [array for _, array in hiddens]
    rows = arrays[0].shape[0]
    full, width = down0.shape

    def body(*refs):
        down_early_kernel(*refs, offsets=offsets, chips=chips)

    return pl.pallas_call(
        body,
        in_specs=[whole(pltpu.SMEM)] + [whole()] * (len(arrays) + 2),
        out_shape=jax.ShapeDtypeStruct((rows, CORES * width), jnp.float32),
        scratch_shapes=[pltpu.VMEM((full, CORES * width), jnp.bfloat16)],
        compiler_params=params(16),
        name="down_early",
    )(place, *arrays, down0, down1)


def down_last_kernel(
    place_ref, total_ref, hidden_ref, down0_ref, down1_ref, out_ref, down_ref, result_ref, *, half
):
    both_columns(place_ref, down0_ref, down1_ref, down_ref)
    total = total_ref[...] + jnp.dot(
        hidden_ref[...], down_ref[...], preferred_element_type=jnp.float32
    )
    result_ref[...] = total.astype(jnp.bfloat16)
    step = GROUP * half
    place = packed_place((GROUP * PAD, step), 0, half)
    for g in range(out_ref.shape[0] // (GROUP * PAD)):
        out_ref[g * GROUP * PAD : (g + 1) * GROUP * PAD, :] = jnp.dot(
            place, result_ref[g * step : (g + 1) * step, :], preferred_element_type=jnp.float32
        ).astype(jnp.bfloat16)


def down_last(place, total, last, down0, down1, chips, half):
    offset, hidden = last
    rows, units = hidden.shape
    _, width = down0.shape

    def body(*refs):
        down_last_kernel(*refs, half=half)

    def chip_rows(place_ref):
        return lax.rem(place_ref[0] + (offset + chips), chips)

    return pl.pallas_call(
        body,
        grid_spec=pltpu.PrefetchScalarGridSpec(
            num_scalar_prefetch=1,
            grid=(1,),
            in_specs=[
                pl.BlockSpec((rows, CORES * width), lambda i, p: (0, 0)),
                pl.BlockSpec((rows, units), lambda i, p: (0, 0)),
                pl.BlockSpec((units, width), lambda i, p: (chip_rows(p), 0)),
                pl.BlockSpec((units, width), lambda i, p: (chip_rows(p), 0)),
            ],
            out_specs=pl.BlockSpec((rows // half * PAD, CORES * width), lambda i, p: (0, 0)),
            scratch_shapes=[
                pltpu.VMEM((units, CORES * width), jnp.bfloat16),
                pltpu.VMEM((rows, CORES * width), jnp.bfloat16),
            ],
        ),
        out_shape=jax.ShapeDtypeStruct((rows // half * PAD, CORES * width), jnp.bfloat16),
        compiler_params=params(8),
        name="down_last",
    )(place, total, hidden, down0, down1)


def combine_kernel(returned_ref, cols_ref, mixed_ref):
    rows, wide = mixed_ref.shape
    slots = returned_ref.shape[0]
    cols = cols_ref[...]
    targets = cols[:, 0:2].astype(jnp.int32)
    slot_index = lax.broadcasted_iota(jnp.int32, (rows, slots), 1)
    returned = returned_ref[...]
    mixed = jnp.zeros((rows, wide), jnp.float32)
    for k in range(2):
        chosen = jnp.where(slot_index == targets[:, k : k + 1], 1.0, 0.0).astype(jnp.bfloat16)
        picked = jnp.dot(chosen, returned, preferred_element_type=jnp.float32)
        mixed = mixed + picked * cols[:, 2 + k : 3 + k]
    mixed_ref[...] = mixed


def combine(returned, cols):
    return pl.pallas_call(
        combine_kernel,
        out_shape=jax.ShapeDtypeStruct((cols.shape[0], returned.shape[1]), jnp.float32),
        compiler_params=params(8),
        name="combine",
    )(returned, cols)


def sums_kernel(place_ref, parts_ref, mixed_ref, sums_ref):
    rows, width = mixed_ref.shape
    both = parts_ref[0] + parts_ref[1]
    for c in range(CORES):

        @pl.when(place_ref[1] == c)
        def _():
            mixed_ref[...] = both[:, c * width : (c + 1) * width]

    sums = jnp.sum(both * both, axis=1, keepdims=True)
    line = jnp.transpose(jnp.broadcast_to(sums, (rows, 128)))[0:1, :]
    for j in range(sums_ref.shape[0]):
        sums_ref[j] = line


def sums_of(place, parts, chips):
    _, rows, wide = parts.shape
    return pl.pallas_call(
        sums_kernel,
        in_specs=[whole(pltpu.SMEM), whole()],
        out_shape=(
            jax.ShapeDtypeStruct((rows, wide // CORES), jnp.float32),
            jax.ShapeDtypeStruct((chips, 1, rows), jnp.float32),
        ),
        compiler_params=params(4),
        name="sums",
    )(place, parts)


def final_kernel(mixed_ref, sums_ref, gain_ref, out_ref):
    rows, width = mixed_ref.shape
    chips = sums_ref.shape[0]
    total = sums_ref[0]
    for j in range(1, chips):
        total = total + sums_ref[j]
    scale = lax.rsqrt(total / (chips * CORES * width) + epsilon)
    column = jnp.transpose(jnp.broadcast_to(scale, (8, rows)))[:, 0:1]
    out_ref[...] = (mixed_ref[...] * column * gain_ref[...]).astype(jnp.bfloat16)


def final(mixed, sums, gain):
    return pl.pallas_call(
        final_kernel,
        out_shape=jax.ShapeDtypeStruct(mixed.shape, jnp.bfloat16),
        compiler_params=params(4),
        name="final",
    )(mixed, sums, gain)


def exchange(value, axis):
    return lax.all_to_all(value, axis, split_axis=0, concat_axis=0, tiled=True)


def blocks_exchange(value):
    wide = value.shape[1]
    return exchange(value.reshape(-1, PAD, wide), "ep").reshape(-1, wide)


def swap(value):
    return lax.ppermute(value, "c", [(0, 1), (1, 0)])


def ring(value):
    chips = lax.axis_size("x")
    onward = [(i, (i + 1) % chips) for i in range(chips)]
    backward = [(i, (i - 1) % chips) for i in range(chips)]
    arrays = [(0, value)]
    before, after = value, value
    for step in range(1, chips // 2 + 1):
        before = lax.ppermute(before, "x", onward)
        arrays.append((-step, before))
        if step < chips - step:
            after = lax.ppermute(after, "x", backward)
            arrays.append((step, after))
    return arrays


def layer(
    tokens, expert_ids, route_weights, pre_gain, post_gain, gate_weight, up_weight, down_weight
):
    tok_rows = tokens.shape[0]
    ep_count = lax.axis_size("ep")
    chips = lax.axis_size("x")
    top_count = expert_ids.shape[1]
    capacity = max(2, tok_rows * top_count * 5 // (4 * ep_count))
    half = capacity // CORES
    place = jnp.stack([lax.axis_index("x"), lax.axis_index("c")]).astype(jnp.int32)
    gate0, up0, down0 = gate_weight[0], up_weight[0], down_weight[0]
    both = lax.all_gather(prepare(in_hbm(tokens), in_hbm(pre_gain[None, :])), "c", axis=0)
    outgoing, cols = dispatch(
        place,
        both,
        in_hbm(jnp.transpose(expert_ids)),
        in_hbm(jnp.transpose(route_weights)),
        ep_count,
        capacity,
    )
    arrived = blocks_exchange(outgoing)
    swapped = []
    for weight in (gate0, up0, down0):
        swapped.append(swap(weight))
    arrived, gate1, up1, down1 = lax.optimization_barrier((arrived, *swapped))
    features = exchange(arrange(arrived, both, chips, half), "x")
    hidden = hidden_of(place, features, gate0, up0, in_hbm(gate1), in_hbm(up1))
    *early, last = ring(hidden)
    total = down_early(place, early, in_hbm(down0), in_hbm(down1), chips)
    result = down_last(place, total, last, in_hbm(down0), in_hbm(down1), chips, half)
    mixed = lax.all_gather(combine(blocks_exchange(result), cols), "c", axis=0)
    mixed, sums = sums_of(place, mixed, chips)
    sums = exchange(sums, "x")
    return final(mixed, sums, in_hbm(post_gain[None, :]))


def solution(mesh):
    ep_count, tp_count = mesh.devices.shape
    devices = mesh.devices.reshape(ep_count, tp_count // CORES, CORES)
    return jax.shard_map(
        layer,
        mesh=Mesh(devices, ("ep", "x", "c")),
        in_specs=(
            P("ep", ("x", "c")),
            P("ep", None),
            P("ep", None),
            P(("x", "c")),
            P(("x", "c")),
            P("ep", None, ("x", "c")),
            P("ep", None, ("x", "c")),
            P("ep", None, ("x", "c")),
        ),
        out_specs=P("ep", ("x", "c")),
        check_vma=False,
    )
```

```python
import jax
import jax.numpy as jnp
from jax import lax
from jax.experimental import pallas as pl
from jax.experimental.pallas import tpu as pltpu
from jax.sharding import Mesh, PartitionSpec as P


epsilon = 1e-06
CORES = 2
PAD = 8
EXTRA = 16
GROUP = 16


def params(mebibytes):
    return pltpu.CompilerParams(vmem_limit_bytes=mebibytes << 20)


def in_hbm(value):
    return pltpu.with_memory_space_constraint(value, pltpu.HBM)


def whole(memory_space=pltpu.VMEM):
    return pl.BlockSpec(memory_space=memory_space)


def prepare_kernel(tok_ref, gain_ref, out_ref):
    rows = tok_ref.shape[0]
    out_ref[0:rows, :] = tok_ref[...]
    gain = gain_ref[...]
    piece0 = gain.astype(jnp.bfloat16).astype(jnp.float32)
    piece1 = (gain - piece0).astype(jnp.bfloat16).astype(jnp.float32)
    piece2 = gain - piece0 - piece1
    empty = jnp.zeros((EXTRA - 3, gain.shape[1]), jnp.float32)
    lines = jnp.concatenate([piece0, piece1, piece2, empty], axis=0)
    out_ref[rows : rows + EXTRA, :] = lines.astype(jnp.bfloat16)


def prepare(tokens, gain):
    rows, width = tokens.shape
    return pl.pallas_call(
        prepare_kernel,
        out_shape=jax.ShapeDtypeStruct((rows + EXTRA, width), jnp.bfloat16),
        compiler_params=params(4),
        name="prepare",
    )(tokens, gain)


def dispatch_kernel(place_ref, tok_ref, ids_ref, weights_ref, out_ref, cols_ref, *, capacity):
    rows = ids_ref.shape[1]
    slots = out_ref.shape[0]
    experts = slots // PAD
    ids = ids_ref[...]
    expert_index = lax.broadcasted_iota(jnp.int32, (experts, rows), 0)
    hot0 = jnp.where(expert_index == ids[0:1, :], 1.0, 0.0)
    hot1 = jnp.where(expert_index == ids[1:2, :], 1.0, 0.0)
    earlier = lax.broadcasted_iota(jnp.int32, (rows, rows), 0) < lax.broadcasted_iota(
        jnp.int32, (rows, rows), 1
    )
    earlier = jnp.where(earlier, 1.0, 0.0).astype(jnp.bfloat16)
    counts = jnp.dot((hot0 + hot1).astype(jnp.bfloat16), earlier, preferred_element_type=jnp.float32)
    half = capacity // CORES
    targets = []
    for k, hot in enumerate((hot0, hot1)):
        slot = jnp.sum(hot * counts, axis=0, keepdims=True).astype(jnp.int32)
        slot = slot - place_ref[1] * half
        mine = jnp.logical_and(slot >= 0, slot < half)
        targets.append(jnp.where(mine, ids[k : k + 1, :] * PAD + slot, -1))
    slot_index = lax.broadcasted_iota(jnp.int32, (slots, rows), 0)
    chosen = jnp.logical_or(slot_index == targets[0], slot_index == targets[1])
    chosen = jnp.where(chosen, 1.0, 0.0).astype(jnp.bfloat16)
    width = tok_ref.shape[2]
    for c in range(CORES):
        out_ref[:, c * width : (c + 1) * width] = jnp.dot(
            chosen, tok_ref[c, 0:rows, :], preferred_element_type=jnp.float32
        ).astype(jnp.bfloat16)
    lines = jnp.concatenate(
        [
            targets[0].astype(jnp.float32),
            targets[1].astype(jnp.float32),
            weights_ref[...],
            jnp.zeros((4, rows), jnp.float32),
        ],
        axis=0,
    )
    cols_ref[...] = jnp.transpose(lines)


def dispatch(place, tokens, ids, weights, experts, capacity):
    rows = ids.shape[1]
    width = tokens.shape[2]

    def body(*refs):
        dispatch_kernel(*refs, capacity=capacity)

    return pl.pallas_call(
        body,
        in_specs=[whole(pltpu.SMEM), whole(), whole(), whole()],
        out_shape=(
            jax.ShapeDtypeStruct((experts * PAD, CORES * width), jnp.bfloat16),
            pltpu.HBM((rows, 8), jnp.float32),
        ),
        compiler_params=params(8),
        name="dispatch",
    )(place, tokens, ids, weights)


def packed_place(shape, slot_axis, capacity):
    padded = lax.broadcasted_iota(jnp.int32, shape, slot_axis)
    packed = lax.broadcasted_iota(jnp.int32, shape, 1 - slot_axis)
    block = padded // PAD
    slot = padded - block * PAD
    same = jnp.logical_and(slot < capacity, packed == block * capacity + slot)
    return jnp.where(same, 1.0, 0.0).astype(jnp.bfloat16)


def arrange_kernel(arrived_ref, tok_ref, out_ref, *, half):
    step = GROUP * half
    width = tok_ref.shape[2]
    first = tok_ref.shape[1] - EXTRA
    rows, _ = out_ref.shape
    place = packed_place((step, GROUP * PAD), 1, half)
    for g in range(arrived_ref.shape[0] // (GROUP * PAD)):
        out_ref[g * step : (g + 1) * step, :] = jnp.dot(
            place,
            arrived_ref[g * GROUP * PAD : (g + 1) * GROUP * PAD, :],
            preferred_element_type=jnp.float32,
        ).astype(jnp.bfloat16)
    for c in range(CORES):
        out_ref[rows - EXTRA :, c * width : (c + 1) * width] = tok_ref[
            c, first : first + EXTRA, :
        ]


def arrange(arrived, tokens, half):
    blocks = arrived.shape[0] // PAD
    width = arrived.shape[1]

    def body(*refs):
        arrange_kernel(*refs, half=half)

    return pl.pallas_call(
        body,
        out_shape=jax.ShapeDtypeStruct((blocks * half + EXTRA, width), jnp.bfloat16),
        compiler_params=params(8),
        name="arrange",
    )(arrived, tokens)


def gained(feat_ref):
    rows = feat_ref.shape[0] - EXTRA
    pieces = feat_ref[rows:, :].astype(jnp.float32)
    gain = pieces[0:1, :] + pieces[1:2, :] + pieces[2:3, :]
    part = feat_ref[0:rows, :].astype(jnp.float32)
    return (part * gain).astype(jnp.bfloat16), part * part


def chip_at(place_ref, offset, chips):
    return lax.rem(place_ref[0] + (offset + chips), chips)


def gate_early_kernel(*refs, offsets, last, chips):
    count = len(offsets)
    place_ref, *rest = refs
    feat_refs, weight_refs = rest[:count], rest[count : count + 4]
    total_refs, (squares_ref, rows_ref) = rest[count + 4 : count + 8], rest[count + 8 :]
    wide = feat_refs[0].shape[1]
    totals = [jnp.zeros(ref.shape, jnp.float32) for ref in total_refs]
    squares = jnp.zeros(squares_ref.shape, jnp.float32)
    for offset, feat_ref in zip(offsets, feat_refs):
        begin = pl.multiple_of(chip_at(place_ref, offset, chips) * wide, wide)
        part, square = gained(feat_ref)
        squares = squares + square
        for i, weight_ref in enumerate(weight_refs):
            totals[i] = totals[i] + jnp.dot(
                part, weight_ref[pl.ds(begin, wide), :], preferred_element_type=jnp.float32
            )
    for i, total in enumerate(totals):
        total_refs[i][...] = total
    squares_ref[...] = squares
    begin = pl.multiple_of(chip_at(place_ref, last, chips) * wide, wide)
    for i, weight_ref in enumerate(weight_refs):
        rows_ref[i] = weight_ref[pl.ds(begin, wide), :]


def gate_early(place, features, last, weights, chips):
    offsets = [offset for offset, _ in features]
    arrays = [array for _, array in features]
    rows, wide = arrays[0].shape
    rows = rows - EXTRA
    units = weights[0].shape[1]

    def body(*refs):
        gate_early_kernel(*refs, offsets=offsets, last=last, chips=chips)

    total = jax.ShapeDtypeStruct((rows, units), jnp.float32)
    return pl.pallas_call(
        body,
        in_specs=[whole(pltpu.SMEM)] + [whole()] * (len(arrays) + 4),
        out_shape=(
            *[total] * 4,
            jax.ShapeDtypeStruct((rows, wide), jnp.float32),
            jax.ShapeDtypeStruct((4, wide, units), jnp.bfloat16),
        ),
        compiler_params=params(16),
        name="gate_early",
    )(place, *arrays, *weights)


def gate_last_kernel(place_ref, *refs, chips):
    total_refs, (squares_ref, rows_ref, feat_ref, out_ref) = refs[:4], refs[4:]
    units = rows_ref.shape[2]
    part, square = gained(feat_ref)
    square = squares_ref[...] + square
    full = chips * square.shape[1]
    scale = lax.rsqrt(jnp.sum(square, axis=1, keepdims=True) / full + epsilon)
    totals = [
        scale * (ref[...] + jnp.dot(part, rows_ref[i], preferred_element_type=jnp.float32))
        for i, ref in enumerate(total_refs)
    ]

    def hidden_of(gate, upper):
        return (gate / (1.0 + jnp.exp(-gate)) * upper).astype(jnp.bfloat16)

    own = hidden_of(totals[0], totals[1])
    other = hidden_of(totals[2], totals[3])
    for c in range(CORES):

        @pl.when(place_ref[1] == c)
        def _():
            out_ref[:, c * units : (c + 1) * units] = own
            out_ref[:, (1 - c) * units : (2 - c) * units] = other


def gate_last(place, early, feature, chips):
    rows, units = early[0].shape

    def body(*refs):
        gate_last_kernel(*refs, chips=chips)

    return pl.pallas_call(
        body,
        in_specs=[whole(pltpu.SMEM)] + [whole()] * 7,
        out_shape=jax.ShapeDtypeStruct((rows, CORES * units), jnp.bfloat16),
        compiler_params=params(16),
        name="gate_last",
    )(place, *early, feature)


def both_columns(place_ref, down0_ref, down1_ref, down_ref):
    width = down0_ref.shape[1]
    for c in range(CORES):

        @pl.when(place_ref[1] == c)
        def _():
            down_ref[:, c * width : (c + 1) * width] = down0_ref[...]
            down_ref[:, (1 - c) * width : (2 - c) * width] = down1_ref[...]


def down_early_kernel(*refs, offsets, last, chips):
    place_ref, *hidden_refs, down0_ref, down1_ref, out_ref, rows_ref, down_ref = refs
    _, units = hidden_refs[0].shape
    both_columns(place_ref, down0_ref, down1_ref, down_ref)
    total = jnp.zeros(out_ref.shape, jnp.float32)
    for offset, ref in zip(offsets, hidden_refs):
        begin = pl.multiple_of(chip_at(place_ref, offset, chips) * units, units)
        total = total + jnp.dot(
            ref[...], down_ref[pl.ds(begin, units), :], preferred_element_type=jnp.float32
        )
    out_ref[...] = total
    begin = pl.multiple_of(chip_at(place_ref, last, chips) * units, units)
    rows_ref[...] = down_ref[pl.ds(begin, units), :]


def down_early(place, hiddens, last, down0, down1, chips):
    offsets = [offset for offset, _ in hiddens]
    arrays = [array for _, array in hiddens]
    rows, units = arrays[0].shape
    full, width = down0.shape

    def body(*refs):
        down_early_kernel(*refs, offsets=offsets, last=last, chips=chips)

    return pl.pallas_call(
        body,
        in_specs=[whole(pltpu.SMEM)] + [whole()] * (len(arrays) + 2),
        out_shape=(
            jax.ShapeDtypeStruct((rows, CORES * width), jnp.float32),
            jax.ShapeDtypeStruct((units, CORES * width), jnp.bfloat16),
        ),
        scratch_shapes=[pltpu.VMEM((full, CORES * width), jnp.bfloat16)],
        compiler_params=params(16),
        name="down_early",
    )(place, *arrays, down0, down1)


def down_last_kernel(total_ref, rows_ref, hidden_ref, out_ref, result_ref, *, half):
    total = total_ref[...] + jnp.dot(
        hidden_ref[...], rows_ref[...], preferred_element_type=jnp.float32
    )
    result_ref[...] = total.astype(jnp.bfloat16)
    step = GROUP * half
    place = packed_place((GROUP * PAD, step), 0, half)
    for g in range(out_ref.shape[0] // (GROUP * PAD)):
        out_ref[g * GROUP * PAD : (g + 1) * GROUP * PAD, :] = jnp.dot(
            place, result_ref[g * step : (g + 1) * step, :], preferred_element_type=jnp.float32
        ).astype(jnp.bfloat16)


def down_last(early, hidden, half):
    rows, wide = early[0].shape

    def body(*refs):
        down_last_kernel(*refs, half=half)

    return pl.pallas_call(
        body,
        out_shape=jax.ShapeDtypeStruct((rows // half * PAD, wide), jnp.bfloat16),
        scratch_shapes=[pltpu.VMEM((rows, wide), jnp.bfloat16)],
        compiler_params=params(8),
        name="down_last",
    )(*early, hidden)


def combine_kernel(returned_ref, cols_ref, mixed_ref):
    rows, wide = mixed_ref.shape
    slots = returned_ref.shape[0]
    cols = cols_ref[...]
    targets = cols[:, 0:2].astype(jnp.int32)
    slot_index = lax.broadcasted_iota(jnp.int32, (rows, slots), 1)
    returned = returned_ref[...]
    mixed = jnp.zeros((rows, wide), jnp.float32)
    for k in range(2):
        chosen = jnp.where(slot_index == targets[:, k : k + 1], 1.0, 0.0).astype(jnp.bfloat16)
        picked = jnp.dot(chosen, returned, preferred_element_type=jnp.float32)
        mixed = mixed + picked * cols[:, 2 + k : 3 + k]
    mixed_ref[...] = mixed


def combine(returned, cols):
    return pl.pallas_call(
        combine_kernel,
        out_shape=jax.ShapeDtypeStruct((cols.shape[0], returned.shape[1]), jnp.float32),
        compiler_params=params(8),
        name="combine",
    )(returned, cols)


def sums_kernel(place_ref, parts_ref, mixed_ref, sums_ref):
    rows, width = mixed_ref.shape
    both = parts_ref[0] + parts_ref[1]
    for c in range(CORES):

        @pl.when(place_ref[1] == c)
        def _():
            mixed_ref[...] = both[:, c * width : (c + 1) * width]

    sums = jnp.sum(both * both, axis=1, keepdims=True)
    line = jnp.transpose(jnp.broadcast_to(sums, (rows, 128)))[0:1, :]
    for j in range(sums_ref.shape[0]):
        sums_ref[j] = line


def sums_of(place, parts, chips):
    _, rows, wide = parts.shape
    return pl.pallas_call(
        sums_kernel,
        in_specs=[whole(pltpu.SMEM), whole()],
        out_shape=(
            jax.ShapeDtypeStruct((rows, wide // CORES), jnp.float32),
            jax.ShapeDtypeStruct((chips, 1, rows), jnp.float32),
        ),
        compiler_params=params(4),
        name="sums",
    )(place, parts)


def final_kernel(mixed_ref, sums_ref, gain_ref, out_ref):
    rows, width = mixed_ref.shape
    chips = sums_ref.shape[0]
    total = sums_ref[0]
    for j in range(1, chips):
        total = total + sums_ref[j]
    scale = lax.rsqrt(total / (chips * CORES * width) + epsilon)
    column = jnp.transpose(jnp.broadcast_to(scale, (8, rows)))[:, 0:1]
    out_ref[...] = (mixed_ref[...] * column * gain_ref[...]).astype(jnp.bfloat16)


def final(mixed, sums, gain):
    return pl.pallas_call(
        final_kernel,
        out_shape=jax.ShapeDtypeStruct(mixed.shape, jnp.bfloat16),
        compiler_params=params(4),
        name="final",
    )(mixed, sums, gain)


def exchange(value, axis):
    return lax.all_to_all(value, axis, split_axis=0, concat_axis=0, tiled=True)


def blocks_exchange(value):
    wide = value.shape[1]
    return exchange(value.reshape(-1, PAD, wide), "ep").reshape(-1, wide)


def swap(value):
    return lax.ppermute(value, "c", [(0, 1), (1, 0)])


def ring(value):
    chips = lax.axis_size("x")
    onward = [(i, (i + 1) % chips) for i in range(chips)]
    backward = [(i, (i - 1) % chips) for i in range(chips)]
    arrays = [(0, value)]
    before, after = value, value
    for step in range(1, chips // 2 + 1):
        before = lax.ppermute(before, "x", onward)
        arrays.append((-step, before))
        if step < chips - step:
            after = lax.ppermute(after, "x", backward)
            arrays.append((step, after))
    return arrays


def layer(
    tokens, expert_ids, route_weights, pre_gain, post_gain, gate_weight, up_weight, down_weight
):
    tok_rows = tokens.shape[0]
    ep_count = lax.axis_size("ep")
    chips = lax.axis_size("x")
    top_count = expert_ids.shape[1]
    capacity = max(2, tok_rows * top_count * 5 // (4 * ep_count))
    half = capacity // CORES
    place = jnp.stack([lax.axis_index("x"), lax.axis_index("c")]).astype(jnp.int32)
    gate0, up0, down0 = gate_weight[0], up_weight[0], down_weight[0]
    both = lax.all_gather(prepare(in_hbm(tokens), in_hbm(pre_gain[None, :])), "c", axis=0)
    outgoing, cols = dispatch(
        place,
        both,
        in_hbm(jnp.transpose(expert_ids)),
        in_hbm(jnp.transpose(route_weights)),
        ep_count,
        capacity,
    )
    arrived = blocks_exchange(outgoing)
    swapped = []
    for weight in (gate0, up0, down0):
        swapped.append(swap(weight))
    arrived, gate1, up1, down1 = lax.optimization_barrier((arrived, *swapped))
    *early, (last, feature) = ring(arrange(arrived, both, half))
    weights = (gate0, up0, in_hbm(gate1), in_hbm(up1))
    projected = gate_early(place, early, last, weights, chips)
    *early, (last, hidden) = ring(gate_last(place, projected, feature, chips))
    summed = down_early(place, early, last, in_hbm(down0), in_hbm(down1), chips)
    result = down_last(summed, hidden, half)
    mixed = lax.all_gather(combine(blocks_exchange(result), cols), "c", axis=0)
    mixed, sums = sums_of(place, mixed, chips)
    sums = exchange(sums, "x")
    return final(mixed, sums, in_hbm(post_gain[None, :]))


def solution(mesh):
    ep_count, tp_count = mesh.devices.shape
    devices = mesh.devices.reshape(ep_count, tp_count // CORES, CORES)
    return jax.shard_map(
        layer,
        mesh=Mesh(devices, ("ep", "x", "c")),
        in_specs=(
            P("ep", ("x", "c")),
            P("ep", None),
            P("ep", None),
            P(("x", "c")),
            P(("x", "c")),
            P("ep", None, ("x", "c")),
            P("ep", None, ("x", "c")),
            P("ep", None, ("x", "c")),
        ),
        out_specs=P("ep", ("x", "c")),
        check_vma=False,
    )
```

```python
import jax
import jax.numpy as jnp
from jax import lax
from jax.experimental import pallas as pl
from jax.experimental.pallas import tpu as pltpu
from jax.sharding import Mesh, PartitionSpec as P


epsilon = 1e-06
CORES = 2
PAD = 8
EXTRA = 16
GROUP = 16


def params(mebibytes):
    return pltpu.CompilerParams(vmem_limit_bytes=mebibytes << 20)


def in_hbm(value):
    return pltpu.with_memory_space_constraint(value, pltpu.HBM)


def whole(memory_space=pltpu.VMEM):
    return pl.BlockSpec(memory_space=memory_space)


def prepare_kernel(tok_ref, gain_ref, out_ref):
    rows = tok_ref.shape[0]
    out_ref[0:rows, :] = tok_ref[...]
    gain = gain_ref[...]
    piece0 = gain.astype(jnp.bfloat16).astype(jnp.float32)
    piece1 = (gain - piece0).astype(jnp.bfloat16).astype(jnp.float32)
    piece2 = gain - piece0 - piece1
    empty = jnp.zeros((EXTRA - 3, gain.shape[1]), jnp.float32)
    lines = jnp.concatenate([piece0, piece1, piece2, empty], axis=0)
    out_ref[rows : rows + EXTRA, :] = lines.astype(jnp.bfloat16)


def prepare(tokens, gain):
    rows, width = tokens.shape
    return pl.pallas_call(
        prepare_kernel,
        out_shape=jax.ShapeDtypeStruct((rows + EXTRA, width), jnp.bfloat16),
        compiler_params=params(4),
        name="prepare",
    )(tokens, gain)


def dispatch_kernel(place_ref, tok_ref, ids_ref, weights_ref, out_ref, cols_ref, *, capacity):
    rows = ids_ref.shape[1]
    slots = out_ref.shape[0]
    experts = slots // PAD
    ids = ids_ref[...]
    expert_index = lax.broadcasted_iota(jnp.int32, (experts, rows), 0)
    hot0 = jnp.where(expert_index == ids[0:1, :], 1.0, 0.0)
    hot1 = jnp.where(expert_index == ids[1:2, :], 1.0, 0.0)
    earlier = lax.broadcasted_iota(jnp.int32, (rows, rows), 0) < lax.broadcasted_iota(
        jnp.int32, (rows, rows), 1
    )
    earlier = jnp.where(earlier, 1.0, 0.0).astype(jnp.bfloat16)
    counts = jnp.dot((hot0 + hot1).astype(jnp.bfloat16), earlier, preferred_element_type=jnp.float32)
    half = capacity // CORES
    targets = []
    for k, hot in enumerate((hot0, hot1)):
        slot = jnp.sum(hot * counts, axis=0, keepdims=True).astype(jnp.int32)
        slot = slot - place_ref[1] * half
        mine = jnp.logical_and(slot >= 0, slot < half)
        targets.append(jnp.where(mine, ids[k : k + 1, :] * PAD + slot, -1))
    slot_index = lax.broadcasted_iota(jnp.int32, (slots, rows), 0)
    chosen = jnp.logical_or(slot_index == targets[0], slot_index == targets[1])
    chosen = jnp.where(chosen, 1.0, 0.0).astype(jnp.bfloat16)
    width = tok_ref.shape[2]
    for c in range(CORES):
        out_ref[:, c * width : (c + 1) * width] = jnp.dot(
            chosen, tok_ref[c, 0:rows, :], preferred_element_type=jnp.float32
        ).astype(jnp.bfloat16)
    lines = jnp.concatenate(
        [
            targets[0].astype(jnp.float32),
            targets[1].astype(jnp.float32),
            weights_ref[...],
            jnp.zeros((4, rows), jnp.float32),
        ],
        axis=0,
    )
    cols_ref[...] = jnp.transpose(lines)


def dispatch(place, tokens, ids, weights, experts, capacity):
    rows = ids.shape[1]
    width = tokens.shape[2]

    def body(*refs):
        dispatch_kernel(*refs, capacity=capacity)

    return pl.pallas_call(
        body,
        in_specs=[whole(pltpu.SMEM), whole(), whole(), whole()],
        out_shape=(
            jax.ShapeDtypeStruct((experts * PAD, CORES * width), jnp.bfloat16),
            pltpu.HBM((rows, 8), jnp.float32),
        ),
        compiler_params=params(8),
        name="dispatch",
    )(place, tokens, ids, weights)


def packed_place(shape, slot_axis, capacity):
    padded = lax.broadcasted_iota(jnp.int32, shape, slot_axis)
    packed = lax.broadcasted_iota(jnp.int32, shape, 1 - slot_axis)
    block = padded // PAD
    slot = padded - block * PAD
    same = jnp.logical_and(slot < capacity, packed == block * capacity + slot)
    return jnp.where(same, 1.0, 0.0).astype(jnp.bfloat16)


def arrange_kernel(arrived_ref, tok_ref, out_ref, *, half):
    step = GROUP * half
    width = tok_ref.shape[2]
    first = tok_ref.shape[1] - EXTRA
    rows, _ = out_ref.shape
    place = packed_place((step, GROUP * PAD), 1, half)
    for g in range(arrived_ref.shape[0] // (GROUP * PAD)):
        out_ref[g * step : (g + 1) * step, :] = jnp.dot(
            place,
            arrived_ref[g * GROUP * PAD : (g + 1) * GROUP * PAD, :],
            preferred_element_type=jnp.float32,
        ).astype(jnp.bfloat16)
    for c in range(CORES):
        out_ref[rows - EXTRA :, c * width : (c + 1) * width] = tok_ref[
            c, first : first + EXTRA, :
        ]


def arrange(arrived, tokens, half):
    blocks = arrived.shape[0] // PAD
    width = arrived.shape[1]

    def body(*refs):
        arrange_kernel(*refs, half=half)

    return pl.pallas_call(
        body,
        out_shape=jax.ShapeDtypeStruct((blocks * half + EXTRA, width), jnp.bfloat16),
        compiler_params=params(8),
        name="arrange",
    )(arrived, tokens)


def chip_at(place_ref, offset, chips):
    return lax.rem(place_ref[0] + (offset + chips), chips)


def squares_kernel(*refs):
    *feat_refs, out_ref = refs
    rows = out_ref.shape[0]
    total = jnp.zeros(out_ref.shape, jnp.float32)
    for ref in feat_refs:
        part = ref[0:rows, :].astype(jnp.float32)
        total = total + part * part
    out_ref[...] = total


def squares_of(arrays):
    rows, wide = arrays[0].shape
    return pl.pallas_call(
        squares_kernel,
        out_shape=jax.ShapeDtypeStruct((rows - EXTRA, wide), jnp.float32),
        compiler_params=params(8),
        name="squares",
    )(*arrays)


def hidden_kernel(*refs, offsets):
    chips = len(offsets)
    place_ref, squares_ref, *rest = refs
    feat_refs, weight_refs, (out_ref, normed_ref) = rest[:chips], rest[chips:-2], rest[-2:]
    rows, wide = squares_ref.shape
    units = weight_refs[0].shape[1]
    part = feat_refs[-1][0:rows, :].astype(jnp.float32)
    total = squares_ref[...] + part * part
    scale = lax.rsqrt(jnp.sum(total, axis=1, keepdims=True) / (chips * wide) + epsilon)
    for offset, ref in zip(offsets, feat_refs):
        begin = pl.multiple_of(chip_at(place_ref, offset, chips) * wide, wide)
        pieces = ref[rows:, :].astype(jnp.float32)
        gain = pieces[0:1, :] + pieces[1:2, :] + pieces[2:3, :]
        part = ref[0:rows, :].astype(jnp.float32)
        normed_ref[:, pl.ds(begin, wide)] = (part * scale * gain).astype(jnp.bfloat16)

    def hidden_from(gate_ref, up_ref):
        normed = normed_ref[...]
        gate = jnp.dot(normed, gate_ref[...], preferred_element_type=jnp.float32)
        upper = jnp.dot(normed, up_ref[...], preferred_element_type=jnp.float32)
        return (gate / (1.0 + jnp.exp(-gate)) * upper).astype(jnp.bfloat16)

    own = hidden_from(weight_refs[0], weight_refs[1])
    other = hidden_from(weight_refs[2], weight_refs[3])
    for c in range(CORES):

        @pl.when(place_ref[1] == c)
        def _():
            out_ref[:, c * units : (c + 1) * units] = own
            out_ref[:, (1 - c) * units : (2 - c) * units] = other


def hidden_of(place, squares, features, weights):
    offsets = [offset for offset, _ in features]
    arrays = [array for _, array in features]
    rows, wide = squares.shape
    units = weights[0].shape[1]

    def body(*refs):
        hidden_kernel(*refs, offsets=offsets)

    return pl.pallas_call(
        body,
        in_specs=[whole(pltpu.SMEM)] + [whole()] * (1 + len(arrays) + len(weights)),
        out_shape=jax.ShapeDtypeStruct((rows, CORES * units), jnp.bfloat16),
        scratch_shapes=[pltpu.VMEM((rows, len(arrays) * wide), jnp.bfloat16)],
        compiler_params=params(16),
        name="hidden",
    )(place, squares, *arrays, *weights)


def both_columns(place_ref, down0_ref, down1_ref, down_ref):
    width = down0_ref.shape[1]
    for c in range(CORES):

        @pl.when(place_ref[1] == c)
        def _():
            down_ref[:, c * width : (c + 1) * width] = down0_ref[...]
            down_ref[:, (1 - c) * width : (2 - c) * width] = down1_ref[...]


def down_early_kernel(*refs, offsets, last, chips):
    place_ref, *hidden_refs, down0_ref, down1_ref, out_ref, rows_ref, down_ref = refs
    _, units = hidden_refs[0].shape
    both_columns(place_ref, down0_ref, down1_ref, down_ref)
    total = jnp.zeros(out_ref.shape, jnp.float32)
    for offset, ref in zip(offsets, hidden_refs):
        begin = pl.multiple_of(chip_at(place_ref, offset, chips) * units, units)
        total = total + jnp.dot(
            ref[...], down_ref[pl.ds(begin, units), :], preferred_element_type=jnp.float32
        )
    out_ref[...] = total
    begin = pl.multiple_of(chip_at(place_ref, last, chips) * units, units)
    rows_ref[...] = down_ref[pl.ds(begin, units), :]


def down_early(place, hiddens, last, down0, down1, chips):
    offsets = [offset for offset, _ in hiddens]
    arrays = [array for _, array in hiddens]
    rows, units = arrays[0].shape
    full, width = down0.shape

    def body(*refs):
        down_early_kernel(*refs, offsets=offsets, last=last, chips=chips)

    return pl.pallas_call(
        body,
        in_specs=[whole(pltpu.SMEM)] + [whole()] * (len(arrays) + 2),
        out_shape=(
            jax.ShapeDtypeStruct((rows, CORES * width), jnp.float32),
            jax.ShapeDtypeStruct((units, CORES * width), jnp.bfloat16),
        ),
        scratch_shapes=[pltpu.VMEM((full, CORES * width), jnp.bfloat16)],
        compiler_params=params(16),
        name="down_early",
    )(place, *arrays, down0, down1)


def down_last_kernel(total_ref, rows_ref, hidden_ref, out_ref, result_ref, *, half):
    total = total_ref[...] + jnp.dot(
        hidden_ref[...], rows_ref[...], preferred_element_type=jnp.float32
    )
    result_ref[...] = total.astype(jnp.bfloat16)
    step = GROUP * half
    place = packed_place((GROUP * PAD, step), 0, half)
    for g in range(out_ref.shape[0] // (GROUP * PAD)):
        out_ref[g * GROUP * PAD : (g + 1) * GROUP * PAD, :] = jnp.dot(
            place, result_ref[g * step : (g + 1) * step, :], preferred_element_type=jnp.float32
        ).astype(jnp.bfloat16)


def down_last(early, hidden, half):
    rows, wide = early[0].shape

    def body(*refs):
        down_last_kernel(*refs, half=half)

    return pl.pallas_call(
        body,
        out_shape=jax.ShapeDtypeStruct((rows // half * PAD, wide), jnp.bfloat16),
        scratch_shapes=[pltpu.VMEM((rows, wide), jnp.bfloat16)],
        compiler_params=params(8),
        name="down_last",
    )(*early, hidden)


def combine_kernel(returned_ref, cols_ref, mixed_ref):
    rows, wide = mixed_ref.shape
    slots = returned_ref.shape[0]
    cols = cols_ref[...]
    targets = cols[:, 0:2].astype(jnp.int32)
    slot_index = lax.broadcasted_iota(jnp.int32, (rows, slots), 1)
    returned = returned_ref[...]
    mixed = jnp.zeros((rows, wide), jnp.float32)
    for k in range(2):
        chosen = jnp.where(slot_index == targets[:, k : k + 1], 1.0, 0.0).astype(jnp.bfloat16)
        picked = jnp.dot(chosen, returned, preferred_element_type=jnp.float32)
        mixed = mixed + picked * cols[:, 2 + k : 3 + k]
    mixed_ref[...] = mixed


def combine(returned, cols):
    return pl.pallas_call(
        combine_kernel,
        out_shape=jax.ShapeDtypeStruct((cols.shape[0], returned.shape[1]), jnp.float32),
        compiler_params=params(8),
        name="combine",
    )(returned, cols)


def sums_kernel(place_ref, parts_ref, mixed_ref, sums_ref):
    rows, width = mixed_ref.shape
    both = parts_ref[0] + parts_ref[1]
    for c in range(CORES):

        @pl.when(place_ref[1] == c)
        def _():
            mixed_ref[...] = both[:, c * width : (c + 1) * width]

    sums = jnp.sum(both * both, axis=1, keepdims=True)
    line = jnp.transpose(jnp.broadcast_to(sums, (rows, 128)))[0:1, :]
    for j in range(sums_ref.shape[0]):
        sums_ref[j] = line


def sums_of(place, parts, chips):
    _, rows, wide = parts.shape
    return pl.pallas_call(
        sums_kernel,
        in_specs=[whole(pltpu.SMEM), whole()],
        out_shape=(
            jax.ShapeDtypeStruct((rows, wide // CORES), jnp.float32),
            jax.ShapeDtypeStruct((chips, 1, rows), jnp.float32),
        ),
        compiler_params=params(4),
        name="sums",
    )(place, parts)


def final_kernel(mixed_ref, sums_ref, gain_ref, out_ref):
    rows, width = mixed_ref.shape
    chips = sums_ref.shape[0]
    total = sums_ref[0]
    for j in range(1, chips):
        total = total + sums_ref[j]
    scale = lax.rsqrt(total / (chips * CORES * width) + epsilon)
    column = jnp.transpose(jnp.broadcast_to(scale, (8, rows)))[:, 0:1]
    out_ref[...] = (mixed_ref[...] * column * gain_ref[...]).astype(jnp.bfloat16)


def final(mixed, sums, gain):
    return pl.pallas_call(
        final_kernel,
        out_shape=jax.ShapeDtypeStruct(mixed.shape, jnp.bfloat16),
        compiler_params=params(4),
        name="final",
    )(mixed, sums, gain)


def exchange(value, axis):
    return lax.all_to_all(value, axis, split_axis=0, concat_axis=0, tiled=True)


def blocks_exchange(value):
    wide = value.shape[1]
    return exchange(value.reshape(-1, PAD, wide), "ep").reshape(-1, wide)


def swap(value):
    return lax.ppermute(value, "c", [(0, 1), (1, 0)])


def ring(value):
    chips = lax.axis_size("x")
    onward = [(i, (i + 1) % chips) for i in range(chips)]
    backward = [(i, (i - 1) % chips) for i in range(chips)]
    arrays = [(0, value)]
    before, after = value, value
    for step in range(1, chips // 2 + 1):
        before = lax.ppermute(before, "x", onward)
        arrays.append((-step, before))
        if step < chips - step:
            after = lax.ppermute(after, "x", backward)
            arrays.append((step, after))
    return arrays


def layer(
    tokens, expert_ids, route_weights, pre_gain, post_gain, gate_weight, up_weight, down_weight
):
    tok_rows = tokens.shape[0]
    ep_count = lax.axis_size("ep")
    chips = lax.axis_size("x")
    top_count = expert_ids.shape[1]
    capacity = max(2, tok_rows * top_count * 5 // (4 * ep_count))
    half = capacity // CORES
    place = jnp.stack([lax.axis_index("x"), lax.axis_index("c")]).astype(jnp.int32)
    gate0, up0, down0 = gate_weight[0], up_weight[0], down_weight[0]
    both = lax.all_gather(prepare(in_hbm(tokens), in_hbm(pre_gain[None, :])), "c", axis=0)
    outgoing, cols = dispatch(
        place,
        both,
        in_hbm(jnp.transpose(expert_ids)),
        in_hbm(jnp.transpose(route_weights)),
        ep_count,
        capacity,
    )
    arrived = blocks_exchange(outgoing)
    swapped = []
    for weight in (gate0, up0, down0):
        swapped.append(swap(weight))
    arrived, gate1, up1, down1 = lax.optimization_barrier((arrived, *swapped))
    features = ring(arrange(arrived, both, half))
    squares = squares_of([array for _, array in features[:-1]])
    hidden = hidden_of(place, squares, features, (gate0, up0, gate1, up1))
    *early, (last, hidden) = ring(hidden)
    summed = down_early(place, early, last, down0, down1, chips)
    result = down_last(summed, hidden, half)
    mixed = lax.all_gather(combine(blocks_exchange(result), cols), "c", axis=0)
    mixed, sums = sums_of(place, mixed, chips)
    sums = exchange(sums, "x")
    return final(mixed, sums, in_hbm(post_gain[None, :]))


def solution(mesh):
    ep_count, tp_count = mesh.devices.shape
    devices = mesh.devices.reshape(ep_count, tp_count // CORES, CORES)
    return jax.shard_map(
        layer,
        mesh=Mesh(devices, ("ep", "x", "c")),
        in_specs=(
            P("ep", ("x", "c")),
            P("ep", None),
            P("ep", None),
            P(("x", "c")),
            P(("x", "c")),
            P("ep", None, ("x", "c")),
            P("ep", None, ("x", "c")),
            P("ep", None, ("x", "c")),
        ),
        out_specs=P("ep", ("x", "c")),
        check_vma=False,
    )
```

```python
import jax
import jax.numpy as jnp
from jax import lax
from jax.experimental import pallas as pl
from jax.experimental.pallas import tpu as pltpu
from jax.sharding import Mesh, PartitionSpec as P


epsilon = 1e-06
CORES = 2
PAD = 8
EXTRA = 16
GROUP = 16


def params(mebibytes):
    return pltpu.CompilerParams(vmem_limit_bytes=mebibytes << 20)


def in_hbm(value):
    return pltpu.with_memory_space_constraint(value, pltpu.HBM)


def whole(memory_space=pltpu.VMEM):
    return pl.BlockSpec(memory_space=memory_space)


def prepare_kernel(tok_ref, gain_ref, out_ref):
    rows = tok_ref.shape[0]
    out_ref[0:rows, :] = tok_ref[...]
    gain = gain_ref[...]
    piece0 = gain.astype(jnp.bfloat16).astype(jnp.float32)
    piece1 = (gain - piece0).astype(jnp.bfloat16).astype(jnp.float32)
    piece2 = gain - piece0 - piece1
    empty = jnp.zeros((EXTRA - 3, gain.shape[1]), jnp.float32)
    lines = jnp.concatenate([piece0, piece1, piece2, empty], axis=0)
    out_ref[rows : rows + EXTRA, :] = lines.astype(jnp.bfloat16)


def prepare(tokens, gain):
    rows, width = tokens.shape
    return pl.pallas_call(
        prepare_kernel,
        out_shape=jax.ShapeDtypeStruct((rows + EXTRA, width), jnp.bfloat16),
        compiler_params=params(4),
        name="prepare",
    )(tokens, gain)


def dispatch_kernel(place_ref, tok_ref, ids_ref, weights_ref, out_ref, cols_ref, *, capacity):
    rows = ids_ref.shape[1]
    slots = out_ref.shape[0]
    experts = slots // PAD
    ids = ids_ref[...]
    expert_index = lax.broadcasted_iota(jnp.int32, (experts, rows), 0)
    hot0 = jnp.where(expert_index == ids[0:1, :], 1.0, 0.0)
    hot1 = jnp.where(expert_index == ids[1:2, :], 1.0, 0.0)
    earlier = lax.broadcasted_iota(jnp.int32, (rows, rows), 0) < lax.broadcasted_iota(
        jnp.int32, (rows, rows), 1
    )
    earlier = jnp.where(earlier, 1.0, 0.0).astype(jnp.bfloat16)
    counts = jnp.dot((hot0 + hot1).astype(jnp.bfloat16), earlier, preferred_element_type=jnp.float32)
    half = capacity // CORES
    targets = []
    for k, hot in enumerate((hot0, hot1)):
        slot = jnp.sum(hot * counts, axis=0, keepdims=True).astype(jnp.int32)
        slot = slot - place_ref[1] * half
        mine = jnp.logical_and(slot >= 0, slot < half)
        targets.append(jnp.where(mine, ids[k : k + 1, :] * PAD + slot, -1))
    slot_index = lax.broadcasted_iota(jnp.int32, (slots, rows), 0)
    chosen = jnp.logical_or(slot_index == targets[0], slot_index == targets[1])
    chosen = jnp.where(chosen, 1.0, 0.0).astype(jnp.bfloat16)
    width = tok_ref.shape[2]
    for c in range(CORES):
        out_ref[:, c * width : (c + 1) * width] = jnp.dot(
            chosen, tok_ref[c, 0:rows, :], preferred_element_type=jnp.float32
        ).astype(jnp.bfloat16)
    lines = jnp.concatenate(
        [
            targets[0].astype(jnp.float32),
            targets[1].astype(jnp.float32),
            weights_ref[...],
            jnp.zeros((4, rows), jnp.float32),
        ],
        axis=0,
    )
    cols_ref[...] = jnp.transpose(lines)


def dispatch(place, tokens, ids, weights, experts, capacity):
    rows = ids.shape[1]
    width = tokens.shape[2]

    def body(*refs):
        dispatch_kernel(*refs, capacity=capacity)

    return pl.pallas_call(
        body,
        in_specs=[whole(pltpu.SMEM), whole(), whole(), whole()],
        out_shape=(
            jax.ShapeDtypeStruct((experts * PAD, CORES * width), jnp.bfloat16),
            pltpu.HBM((rows, 8), jnp.float32),
        ),
        compiler_params=params(8),
        name="dispatch",
    )(place, tokens, ids, weights)


def packed_place(shape, slot_axis, capacity):
    padded = lax.broadcasted_iota(jnp.int32, shape, slot_axis)
    packed = lax.broadcasted_iota(jnp.int32, shape, 1 - slot_axis)
    block = padded // PAD
    slot = padded - block * PAD
    same = jnp.logical_and(slot < capacity, packed == block * capacity + slot)
    return jnp.where(same, 1.0, 0.0).astype(jnp.bfloat16)


def arrange_kernel(arrived_ref, tok_ref, out_ref, *, half):
    step = GROUP * half
    width = tok_ref.shape[2]
    first = tok_ref.shape[1] - EXTRA
    rows, _ = out_ref.shape
    place = packed_place((step, GROUP * PAD), 1, half)
    for g in range(arrived_ref.shape[0] // (GROUP * PAD)):
        out_ref[g * step : (g + 1) * step, :] = jnp.dot(
            place,
            arrived_ref[g * GROUP * PAD : (g + 1) * GROUP * PAD, :],
            preferred_element_type=jnp.float32,
        ).astype(jnp.bfloat16)
    for c in range(CORES):
        out_ref[rows - EXTRA :, c * width : (c + 1) * width] = tok_ref[
            c, first : first + EXTRA, :
        ]


def arrange(arrived, tokens, half):
    blocks = arrived.shape[0] // PAD
    width = arrived.shape[1]

    def body(*refs):
        arrange_kernel(*refs, half=half)

    return pl.pallas_call(
        body,
        out_shape=jax.ShapeDtypeStruct((blocks * half + EXTRA, width), jnp.bfloat16),
        compiler_params=params(8),
        name="arrange",
    )(arrived, tokens)


def chip_at(place_ref, offset, chips):
    return lax.rem(place_ref[0] + offset * (1 - 2 * place_ref[1]) + chips, chips)


def squares_kernel(*refs):
    *feat_refs, out_ref = refs
    rows = out_ref.shape[0]
    total = jnp.zeros(out_ref.shape, jnp.float32)
    for ref in feat_refs:
        part = ref[0:rows, :].astype(jnp.float32)
        total = total + part * part
    out_ref[...] = total


def squares_of(arrays):
    rows, wide = arrays[0].shape
    return pl.pallas_call(
        squares_kernel,
        out_shape=jax.ShapeDtypeStruct((rows - EXTRA, wide), jnp.float32),
        compiler_params=params(8),
        name="squares",
    )(*arrays)


def hidden_kernel(*refs, offsets):
    chips = len(offsets)
    place_ref, squares_ref, *rest = refs
    feat_refs, weight_refs, (out_ref, normed_ref) = rest[:chips], rest[chips:-2], rest[-2:]
    rows, wide = squares_ref.shape
    units = weight_refs[0].shape[1]
    part = feat_refs[-1][0:rows, :].astype(jnp.float32)
    total = squares_ref[...] + part * part
    scale = lax.rsqrt(jnp.sum(total, axis=1, keepdims=True) / (chips * wide) + epsilon)
    for offset, ref in zip(offsets, feat_refs):
        begin = pl.multiple_of(chip_at(place_ref, offset, chips) * wide, wide)
        pieces = ref[rows:, :].astype(jnp.float32)
        gain = pieces[0:1, :] + pieces[1:2, :] + pieces[2:3, :]
        part = ref[0:rows, :].astype(jnp.float32)
        normed_ref[:, pl.ds(begin, wide)] = (part * scale * gain).astype(jnp.bfloat16)

    def hidden_from(gate_ref, up_ref):
        normed = normed_ref[...]
        gate = jnp.dot(normed, gate_ref[...], preferred_element_type=jnp.float32)
        upper = jnp.dot(normed, up_ref[...], preferred_element_type=jnp.float32)
        return (gate / (1.0 + jnp.exp(-gate)) * upper).astype(jnp.bfloat16)

    own = hidden_from(weight_refs[0], weight_refs[1])
    other = hidden_from(weight_refs[2], weight_refs[3])
    for c in range(CORES):

        @pl.when(place_ref[1] == c)
        def _():
            out_ref[:, c * units : (c + 1) * units] = own
            out_ref[:, (1 - c) * units : (2 - c) * units] = other


def hidden_of(place, squares, features, weights):
    offsets = [offset for offset, _ in features]
    arrays = [array for _, array in features]
    rows, wide = squares.shape
    units = weights[0].shape[1]

    def body(*refs):
        hidden_kernel(*refs, offsets=offsets)

    return pl.pallas_call(
        body,
        in_specs=[whole(pltpu.SMEM)] + [whole()] * (1 + len(arrays) + len(weights)),
        out_shape=jax.ShapeDtypeStruct((rows, CORES * units), jnp.bfloat16),
        scratch_shapes=[pltpu.VMEM((rows, len(arrays) * wide), jnp.bfloat16)],
        compiler_params=params(16),
        name="hidden",
    )(place, squares, *arrays, *weights)


def both_columns(place_ref, down0_ref, down1_ref, down_ref):
    width = down0_ref.shape[1]
    for c in range(CORES):

        @pl.when(place_ref[1] == c)
        def _():
            down_ref[:, c * width : (c + 1) * width] = down0_ref[...]
            down_ref[:, (1 - c) * width : (2 - c) * width] = down1_ref[...]


def down_early_kernel(*refs, offsets, last, chips):
    place_ref, *hidden_refs, down0_ref, down1_ref, out_ref, rows_ref, down_ref = refs
    _, units = hidden_refs[0].shape
    both_columns(place_ref, down0_ref, down1_ref, down_ref)
    total = jnp.zeros(out_ref.shape, jnp.float32)
    for offset, ref in zip(offsets, hidden_refs):
        begin = pl.multiple_of(chip_at(place_ref, offset, chips) * units, units)
        total = total + jnp.dot(
            ref[...], down_ref[pl.ds(begin, units), :], preferred_element_type=jnp.float32
        )
    out_ref[...] = total
    begin = pl.multiple_of(chip_at(place_ref, last, chips) * units, units)
    rows_ref[...] = down_ref[pl.ds(begin, units), :]


def down_early(place, hiddens, last, down0, down1, chips):
    offsets = [offset for offset, _ in hiddens]
    arrays = [array for _, array in hiddens]
    rows, units = arrays[0].shape
    full, width = down0.shape

    def body(*refs):
        down_early_kernel(*refs, offsets=offsets, last=last, chips=chips)

    return pl.pallas_call(
        body,
        in_specs=[whole(pltpu.SMEM)] + [whole()] * (len(arrays) + 2),
        out_shape=(
            jax.ShapeDtypeStruct((rows, CORES * width), jnp.float32),
            jax.ShapeDtypeStruct((units, CORES * width), jnp.bfloat16),
        ),
        scratch_shapes=[pltpu.VMEM((full, CORES * width), jnp.bfloat16)],
        compiler_params=params(16),
        name="down_early",
    )(place, *arrays, down0, down1)


def down_last_kernel(total_ref, rows_ref, hidden_ref, out_ref, result_ref, *, half):
    total = total_ref[...] + jnp.dot(
        hidden_ref[...], rows_ref[...], preferred_element_type=jnp.float32
    )
    result_ref[...] = total.astype(jnp.bfloat16)
    step = GROUP * half
    place = packed_place((GROUP * PAD, step), 0, half)
    for g in range(out_ref.shape[0] // (GROUP * PAD)):
        out_ref[g * GROUP * PAD : (g + 1) * GROUP * PAD, :] = jnp.dot(
            place, result_ref[g * step : (g + 1) * step, :], preferred_element_type=jnp.float32
        ).astype(jnp.bfloat16)


def down_last(early, hidden, half):
    rows, wide = early[0].shape

    def body(*refs):
        down_last_kernel(*refs, half=half)

    return pl.pallas_call(
        body,
        out_shape=jax.ShapeDtypeStruct((rows // half * PAD, wide), jnp.bfloat16),
        scratch_shapes=[pltpu.VMEM((rows, wide), jnp.bfloat16)],
        compiler_params=params(8),
        name="down_last",
    )(*early, hidden)


def combine_kernel(returned_ref, cols_ref, mixed_ref):
    rows, wide = mixed_ref.shape
    slots = returned_ref.shape[0]
    cols = cols_ref[...]
    targets = cols[:, 0:2].astype(jnp.int32)
    slot_index = lax.broadcasted_iota(jnp.int32, (rows, slots), 1)
    returned = returned_ref[...]
    mixed = jnp.zeros((rows, wide), jnp.float32)
    for k in range(2):
        chosen = jnp.where(slot_index == targets[:, k : k + 1], 1.0, 0.0).astype(jnp.bfloat16)
        picked = jnp.dot(chosen, returned, preferred_element_type=jnp.float32)
        mixed = mixed + picked * cols[:, 2 + k : 3 + k]
    mixed_ref[...] = mixed


def combine(returned, cols):
    return pl.pallas_call(
        combine_kernel,
        out_shape=jax.ShapeDtypeStruct((cols.shape[0], returned.shape[1]), jnp.float32),
        compiler_params=params(8),
        name="combine",
    )(returned, cols)


def sums_kernel(place_ref, parts_ref, mixed_ref, sums_ref):
    rows, width = mixed_ref.shape
    both = parts_ref[0] + parts_ref[1]
    for c in range(CORES):

        @pl.when(place_ref[1] == c)
        def _():
            mixed_ref[...] = both[:, c * width : (c + 1) * width]

    sums = jnp.sum(both * both, axis=1, keepdims=True)
    line = jnp.transpose(jnp.broadcast_to(sums, (rows, 128)))[0:1, :]
    for j in range(sums_ref.shape[0]):
        sums_ref[j] = line


def sums_of(place, parts, chips):
    _, rows, wide = parts.shape
    return pl.pallas_call(
        sums_kernel,
        in_specs=[whole(pltpu.SMEM), whole()],
        out_shape=(
            jax.ShapeDtypeStruct((rows, wide // CORES), jnp.float32),
            jax.ShapeDtypeStruct((chips, 1, rows), jnp.float32),
        ),
        compiler_params=params(4),
        name="sums",
    )(place, parts)


def final_kernel(mixed_ref, sums_ref, gain_ref, out_ref):
    rows, width = mixed_ref.shape
    chips = sums_ref.shape[0]
    total = sums_ref[0]
    for j in range(1, chips):
        total = total + sums_ref[j]
    scale = lax.rsqrt(total / (chips * CORES * width) + epsilon)
    column = jnp.transpose(jnp.broadcast_to(scale, (8, rows)))[:, 0:1]
    out_ref[...] = (mixed_ref[...] * column * gain_ref[...]).astype(jnp.bfloat16)


def final(mixed, sums, gain):
    return pl.pallas_call(
        final_kernel,
        out_shape=jax.ShapeDtypeStruct(mixed.shape, jnp.bfloat16),
        compiler_params=params(4),
        name="final",
    )(mixed, sums, gain)


def exchange(value, axis):
    return lax.all_to_all(value, axis, split_axis=0, concat_axis=0, tiled=True)


def blocks_exchange(value):
    wide = value.shape[1]
    return exchange(value.reshape(-1, PAD, wide), "ep").reshape(-1, wide)


def swap(value):
    return lax.ppermute(value, "c", [(0, 1), (1, 0)])


def ring(value):
    chips = lax.axis_size("x")

    def shift(step):
        return [
            (x * CORES + c, (x + step * (1 - 2 * c)) % chips * CORES + c)
            for x in range(chips)
            for c in range(CORES)
        ]

    arrays = [(0, value)]
    before, after = value, value
    for step in range(1, chips // 2 + 1):
        before = lax.ppermute(before, ("x", "c"), shift(1))
        arrays.append((-step, before))
        if step < chips - step:
            after = lax.ppermute(after, ("x", "c"), shift(-1))
            arrays.append((step, after))
    return arrays


def layer(
    tokens, expert_ids, route_weights, pre_gain, post_gain, gate_weight, up_weight, down_weight
):
    tok_rows = tokens.shape[0]
    ep_count = lax.axis_size("ep")
    chips = lax.axis_size("x")
    top_count = expert_ids.shape[1]
    capacity = max(2, tok_rows * top_count * 5 // (4 * ep_count))
    half = capacity // CORES
    place = jnp.stack([lax.axis_index("x"), lax.axis_index("c")]).astype(jnp.int32)
    gate0, up0, down0 = gate_weight[0], up_weight[0], down_weight[0]
    both = lax.all_gather(prepare(in_hbm(tokens), in_hbm(pre_gain[None, :])), "c", axis=0)
    outgoing, cols = dispatch(
        place,
        both,
        in_hbm(jnp.transpose(expert_ids)),
        in_hbm(jnp.transpose(route_weights)),
        ep_count,
        capacity,
    )
    arrived = blocks_exchange(outgoing)
    swapped = []
    for weight in (gate0, up0, down0):
        swapped.append(swap(weight))
    arrived, gate1, up1, down1 = lax.optimization_barrier((arrived, *swapped))
    features = ring(arrange(arrived, both, half))
    squares = squares_of([array for _, array in features[:-1]])
    hidden = hidden_of(place, squares, features, (gate0, up0, gate1, up1))
    *early, (last, hidden) = ring(hidden)
    summed = down_early(place, early, last, down0, down1, chips)
    result = down_last(summed, hidden, half)
    mixed = lax.all_gather(combine(blocks_exchange(result), cols), "c", axis=0)
    mixed, sums = sums_of(place, mixed, chips)
    sums = exchange(sums, "x")
    return final(mixed, sums, in_hbm(post_gain[None, :]))


def solution(mesh):
    ep_count, tp_count = mesh.devices.shape
    devices = mesh.devices.reshape(ep_count, tp_count // CORES, CORES)
    return jax.shard_map(
        layer,
        mesh=Mesh(devices, ("ep", "x", "c")),
        in_specs=(
            P("ep", ("x", "c")),
            P("ep", None),
            P("ep", None),
            P(("x", "c")),
            P(("x", "c")),
            P("ep", None, ("x", "c")),
            P("ep", None, ("x", "c")),
            P("ep", None, ("x", "c")),
        ),
        out_specs=P("ep", ("x", "c")),
        check_vma=False,
    )
```

```python
import jax
import jax.numpy as jnp
from jax import lax
from jax.experimental import pallas as pl
from jax.experimental.pallas import tpu as pltpu
from jax.sharding import Mesh, PartitionSpec as P


epsilon = 1e-06
CORES = 2
PAD = 8
EXTRA = 16
GROUP = 16


def params(mebibytes):
    return pltpu.CompilerParams(vmem_limit_bytes=mebibytes << 20)


def in_hbm(value):
    return pltpu.with_memory_space_constraint(value, pltpu.HBM)


def whole(memory_space=pltpu.VMEM):
    return pl.BlockSpec(memory_space=memory_space)


def prepare_kernel(tok_ref, gain_ref, out_ref):
    rows = tok_ref.shape[0]
    out_ref[0:rows, :] = tok_ref[...]
    gain = gain_ref[...]
    piece0 = gain.astype(jnp.bfloat16).astype(jnp.float32)
    piece1 = (gain - piece0).astype(jnp.bfloat16).astype(jnp.float32)
    piece2 = gain - piece0 - piece1
    empty = jnp.zeros((EXTRA - 3, gain.shape[1]), jnp.float32)
    lines = jnp.concatenate([piece0, piece1, piece2, empty], axis=0)
    out_ref[rows : rows + EXTRA, :] = lines.astype(jnp.bfloat16)


def prepare(tokens, gain):
    rows, width = tokens.shape
    return pl.pallas_call(
        prepare_kernel,
        out_shape=jax.ShapeDtypeStruct((rows + EXTRA, width), jnp.bfloat16),
        compiler_params=params(4),
        name="prepare",
    )(tokens, gain)


def dispatch_kernel(place_ref, tok_ref, ids_ref, weights_ref, out_ref, cols_ref, *, capacity):
    rows = ids_ref.shape[1]
    slots = out_ref.shape[0]
    experts = slots // PAD
    ids = ids_ref[...]
    expert_index = lax.broadcasted_iota(jnp.int32, (experts, rows), 0)
    hot0 = jnp.where(expert_index == ids[0:1, :], 1.0, 0.0)
    hot1 = jnp.where(expert_index == ids[1:2, :], 1.0, 0.0)
    earlier = lax.broadcasted_iota(jnp.int32, (rows, rows), 0) < lax.broadcasted_iota(
        jnp.int32, (rows, rows), 1
    )
    earlier = jnp.where(earlier, 1.0, 0.0).astype(jnp.bfloat16)
    counts = jnp.dot((hot0 + hot1).astype(jnp.bfloat16), earlier, preferred_element_type=jnp.float32)
    half = capacity // CORES
    targets = []
    for k, hot in enumerate((hot0, hot1)):
        slot = jnp.sum(hot * counts, axis=0, keepdims=True).astype(jnp.int32)
        slot = slot - place_ref[1] * half
        mine = jnp.logical_and(slot >= 0, slot < half)
        targets.append(jnp.where(mine, ids[k : k + 1, :] * PAD + slot, -1))
    slot_index = lax.broadcasted_iota(jnp.int32, (slots, rows), 0)
    chosen = jnp.logical_or(slot_index == targets[0], slot_index == targets[1])
    chosen = jnp.where(chosen, 1.0, 0.0).astype(jnp.bfloat16)
    width = tok_ref.shape[2]
    for c in range(CORES):
        out_ref[:, c * width : (c + 1) * width] = jnp.dot(
            chosen, tok_ref[c, 0:rows, :], preferred_element_type=jnp.float32
        ).astype(jnp.bfloat16)
    lines = jnp.concatenate(
        [
            targets[0].astype(jnp.float32),
            targets[1].astype(jnp.float32),
            weights_ref[...],
            jnp.zeros((4, rows), jnp.float32),
        ],
        axis=0,
    )
    cols_ref[...] = jnp.transpose(lines)


def dispatch(place, tokens, ids, weights, experts, capacity):
    rows = ids.shape[1]
    width = tokens.shape[2]

    def body(*refs):
        dispatch_kernel(*refs, capacity=capacity)

    return pl.pallas_call(
        body,
        in_specs=[whole(pltpu.SMEM), whole(), whole(), whole()],
        out_shape=(
            jax.ShapeDtypeStruct((experts * PAD, CORES * width), jnp.bfloat16),
            pltpu.HBM((rows, 8), jnp.float32),
        ),
        compiler_params=params(8),
        name="dispatch",
    )(place, tokens, ids, weights)


def packed_place(shape, slot_axis, capacity):
    padded = lax.broadcasted_iota(jnp.int32, shape, slot_axis)
    packed = lax.broadcasted_iota(jnp.int32, shape, 1 - slot_axis)
    block = padded // PAD
    slot = padded - block * PAD
    same = jnp.logical_and(slot < capacity, packed == block * capacity + slot)
    return jnp.where(same, 1.0, 0.0).astype(jnp.bfloat16)


def arrange_kernel(arrived_ref, tok_ref, out_ref, *, half):
    step = GROUP * half
    width = tok_ref.shape[2]
    first = tok_ref.shape[1] - EXTRA
    rows, _ = out_ref.shape
    place = packed_place((step, GROUP * PAD), 1, half)
    for g in range(arrived_ref.shape[0] // (GROUP * PAD)):
        out_ref[g * step : (g + 1) * step, :] = jnp.dot(
            place,
            arrived_ref[g * GROUP * PAD : (g + 1) * GROUP * PAD, :],
            preferred_element_type=jnp.float32,
        ).astype(jnp.bfloat16)
    for c in range(CORES):
        out_ref[rows - EXTRA :, c * width : (c + 1) * width] = tok_ref[
            c, first : first + EXTRA, :
        ]


def arrange(arrived, tokens, half):
    blocks = arrived.shape[0] // PAD
    width = arrived.shape[1]

    def body(*refs):
        arrange_kernel(*refs, half=half)

    return pl.pallas_call(
        body,
        out_shape=jax.ShapeDtypeStruct((blocks * half + EXTRA, width), jnp.bfloat16),
        compiler_params=params(8),
        name="arrange",
    )(arrived, tokens)


def chip_at(place_ref, offset, chips):
    return lax.rem(place_ref[0] + offset * (1 - 2 * place_ref[1]) + chips, chips)


def blocks_of(refs):
    blocks = []
    for ref in refs:
        blocks += [ref] if len(ref.shape) == 2 else [ref.at[i] for i in range(ref.shape[0])]
    return blocks


def squares_kernel(*refs):
    *feat_refs, out_ref = refs
    rows = out_ref.shape[0]
    total = jnp.zeros(out_ref.shape, jnp.float32)
    for ref in blocks_of(feat_refs):
        part = ref[0:rows, :].astype(jnp.float32)
        total = total + part * part
    out_ref[...] = total


def squares_of(arrays):
    rows, wide = arrays[0].shape
    return pl.pallas_call(
        squares_kernel,
        out_shape=jax.ShapeDtypeStruct((rows - EXTRA, wide), jnp.float32),
        compiler_params=params(8),
        name="squares",
    )(*arrays)


def hidden_kernel(*refs, offsets, count):
    chips = len(offsets)
    place_ref, squares_ref, *rest = refs
    feat_refs, weight_refs, (out_ref, normed_ref) = rest[:count], rest[count:-2], rest[-2:]
    rows, wide = squares_ref.shape
    units = weight_refs[0].shape[1]
    total = squares_ref[...]
    for ref in blocks_of(feat_refs[-1:]):
        part = ref[0:rows, :].astype(jnp.float32)
        total = total + part * part
    scale = lax.rsqrt(jnp.sum(total, axis=1, keepdims=True) / (chips * wide) + epsilon)
    sign = 1 - 2 * lax.rem(place_ref[0] + place_ref[1], 2)
    for offset, ref in zip(offsets, blocks_of(feat_refs)):
        chip = lax.rem(place_ref[0] + offset * sign + chips, chips)
        begin = pl.multiple_of(chip * wide, wide)
        pieces = ref[rows:, :].astype(jnp.float32)
        gain = pieces[0:1, :] + pieces[1:2, :] + pieces[2:3, :]
        part = ref[0:rows, :].astype(jnp.float32)
        normed_ref[:, pl.ds(begin, wide)] = (part * scale * gain).astype(jnp.bfloat16)

    def hidden_from(gate_ref, up_ref):
        normed = normed_ref[...]
        gate = jnp.dot(normed, gate_ref[...], preferred_element_type=jnp.float32)
        upper = jnp.dot(normed, up_ref[...], preferred_element_type=jnp.float32)
        return (gate / (1.0 + jnp.exp(-gate)) * upper).astype(jnp.bfloat16)

    own = hidden_from(weight_refs[0], weight_refs[1])
    other = hidden_from(weight_refs[2], weight_refs[3])
    for c in range(CORES):

        @pl.when(place_ref[1] == c)
        def _():
            out_ref[:, c * units : (c + 1) * units] = own
            out_ref[:, (1 - c) * units : (2 - c) * units] = other


def hidden_of(place, squares, offsets, arrays, weights):
    rows, wide = squares.shape
    units = weights[0].shape[1]

    def body(*refs):
        hidden_kernel(*refs, offsets=offsets, count=len(arrays))

    return pl.pallas_call(
        body,
        in_specs=[whole(pltpu.SMEM)] + [whole()] * (1 + len(arrays) + len(weights)),
        out_shape=jax.ShapeDtypeStruct((rows, CORES * units), jnp.bfloat16),
        scratch_shapes=[pltpu.VMEM((rows, len(offsets) * wide), jnp.bfloat16)],
        compiler_params=params(16),
        name="hidden",
    )(place, squares, *arrays, *weights)


def both_columns(place_ref, down0_ref, down1_ref, down_ref):
    width = down0_ref.shape[1]
    for c in range(CORES):

        @pl.when(place_ref[1] == c)
        def _():
            down_ref[:, c * width : (c + 1) * width] = down0_ref[...]
            down_ref[:, (1 - c) * width : (2 - c) * width] = down1_ref[...]


def down_early_kernel(*refs, offsets, last, chips):
    place_ref, *hidden_refs, down0_ref, down1_ref, out_ref, rows_ref, down_ref = refs
    _, units = hidden_refs[0].shape
    both_columns(place_ref, down0_ref, down1_ref, down_ref)
    total = jnp.zeros(out_ref.shape, jnp.float32)
    for offset, ref in zip(offsets, hidden_refs):
        begin = pl.multiple_of(chip_at(place_ref, offset, chips) * units, units)
        total = total + jnp.dot(
            ref[...], down_ref[pl.ds(begin, units), :], preferred_element_type=jnp.float32
        )
    out_ref[...] = total
    begin = pl.multiple_of(chip_at(place_ref, last, chips) * units, units)
    rows_ref[...] = down_ref[pl.ds(begin, units), :]


def down_early(place, hiddens, last, down0, down1, chips):
    offsets = [offset for offset, _ in hiddens]
    arrays = [array for _, array in hiddens]
    rows, units = arrays[0].shape
    full, width = down0.shape

    def body(*refs):
        down_early_kernel(*refs, offsets=offsets, last=last, chips=chips)

    return pl.pallas_call(
        body,
        in_specs=[whole(pltpu.SMEM)] + [whole()] * (len(arrays) + 2),
        out_shape=(
            jax.ShapeDtypeStruct((rows, CORES * width), jnp.float32),
            jax.ShapeDtypeStruct((units, CORES * width), jnp.bfloat16),
        ),
        scratch_shapes=[pltpu.VMEM((full, CORES * width), jnp.bfloat16)],
        compiler_params=params(16),
        name="down_early",
    )(place, *arrays, down0, down1)


def down_last_kernel(total_ref, rows_ref, hidden_ref, out_ref, result_ref, *, half):
    total = total_ref[...] + jnp.dot(
        hidden_ref[...], rows_ref[...], preferred_element_type=jnp.float32
    )
    result_ref[...] = total.astype(jnp.bfloat16)
    step = GROUP * half
    place = packed_place((GROUP * PAD, step), 0, half)
    for g in range(out_ref.shape[0] // (GROUP * PAD)):
        out_ref[g * GROUP * PAD : (g + 1) * GROUP * PAD, :] = jnp.dot(
            place, result_ref[g * step : (g + 1) * step, :], preferred_element_type=jnp.float32
        ).astype(jnp.bfloat16)


def down_last(early, hidden, half):
    rows, wide = early[0].shape

    def body(*refs):
        down_last_kernel(*refs, half=half)

    return pl.pallas_call(
        body,
        out_shape=jax.ShapeDtypeStruct((rows // half * PAD, wide), jnp.bfloat16),
        scratch_shapes=[pltpu.VMEM((rows, wide), jnp.bfloat16)],
        compiler_params=params(8),
        name="down_last",
    )(*early, hidden)


def combine_kernel(returned_ref, cols_ref, mixed_ref):
    rows, wide = mixed_ref.shape
    slots = returned_ref.shape[0]
    cols = cols_ref[...]
    targets = cols[:, 0:2].astype(jnp.int32)
    slot_index = lax.broadcasted_iota(jnp.int32, (rows, slots), 1)
    returned = returned_ref[...]
    mixed = jnp.zeros((rows, wide), jnp.float32)
    for k in range(2):
        chosen = jnp.where(slot_index == targets[:, k : k + 1], 1.0, 0.0).astype(jnp.bfloat16)
        picked = jnp.dot(chosen, returned, preferred_element_type=jnp.float32)
        mixed = mixed + picked * cols[:, 2 + k : 3 + k]
    mixed_ref[...] = mixed


def combine(returned, cols):
    return pl.pallas_call(
        combine_kernel,
        out_shape=jax.ShapeDtypeStruct((cols.shape[0], returned.shape[1]), jnp.float32),
        compiler_params=params(8),
        name="combine",
    )(returned, cols)


def sums_kernel(place_ref, parts_ref, mixed_ref, sums_ref):
    rows, width = mixed_ref.shape
    both = parts_ref[0] + parts_ref[1]
    for c in range(CORES):

        @pl.when(place_ref[1] == c)
        def _():
            mixed_ref[...] = both[:, c * width : (c + 1) * width]

    sums = jnp.sum(both * both, axis=1, keepdims=True)
    line = jnp.transpose(jnp.broadcast_to(sums, (rows, 128)))[0:1, :]
    for j in range(sums_ref.shape[0]):
        sums_ref[j] = line


def sums_of(place, parts, chips):
    _, rows, wide = parts.shape
    return pl.pallas_call(
        sums_kernel,
        in_specs=[whole(pltpu.SMEM), whole()],
        out_shape=(
            jax.ShapeDtypeStruct((rows, wide // CORES), jnp.float32),
            jax.ShapeDtypeStruct((chips, 1, rows), jnp.float32),
        ),
        compiler_params=params(4),
        name="sums",
    )(place, parts)


def final_kernel(mixed_ref, sums_ref, gain_ref, out_ref):
    rows, width = mixed_ref.shape
    chips = sums_ref.shape[0]
    total = sums_ref[0]
    for j in range(1, chips):
        total = total + sums_ref[j]
    scale = lax.rsqrt(total / (chips * CORES * width) + epsilon)
    column = jnp.transpose(jnp.broadcast_to(scale, (8, rows)))[:, 0:1]
    out_ref[...] = (mixed_ref[...] * column * gain_ref[...]).astype(jnp.bfloat16)


def final(mixed, sums, gain):
    return pl.pallas_call(
        final_kernel,
        out_shape=jax.ShapeDtypeStruct(mixed.shape, jnp.bfloat16),
        compiler_params=params(4),
        name="final",
    )(mixed, sums, gain)


def exchange(value, axis):
    return lax.all_to_all(value, axis, split_axis=0, concat_axis=0, tiled=True)


def blocks_exchange(value):
    wide = value.shape[1]
    return exchange(value.reshape(-1, PAD, wide), "ep").reshape(-1, wide)


def swap(value):
    return lax.ppermute(value, "c", [(0, 1), (1, 0)])


def ring(value):
    chips = lax.axis_size("x")

    def shift(step):
        return [
            (x * CORES + c, (x + step * (1 - 2 * c)) % chips * CORES + c)
            for x in range(chips)
            for c in range(CORES)
        ]

    arrays = [(0, value)]
    before, after = value, value
    for step in range(1, chips // 2 + 1):
        before = lax.ppermute(before, ("x", "c"), shift(1))
        arrays.append((-step, before))
        if step < chips - step:
            after = lax.ppermute(after, ("x", "c"), shift(-1))
            arrays.append((step, after))
    return arrays


def neighbours(value):
    chips = lax.axis_size("x")

    def partner(step):
        return [
            (x * CORES + c, (x + step * (1 - 2 * ((x + c) % 2))) % chips * CORES + c)
            for x in range(chips)
            for c in range(CORES)
        ]

    first = lax.ppermute(value, ("x", "c"), partner(1))
    offsets, arrays = [0, 1], [value, first]
    moving, side, low, high = jnp.stack([value, first]), -1, 1, 2
    while len(offsets) < chips:
        moving = lax.ppermute(moving, ("x", "c"), partner(side))
        arrays.append(moving)
        offsets += [side * low, side * high]
        side, low, high = -side, low + 1, high + 1
    return offsets, arrays


def layer(
    tokens, expert_ids, route_weights, pre_gain, post_gain, gate_weight, up_weight, down_weight
):
    tok_rows = tokens.shape[0]
    ep_count = lax.axis_size("ep")
    chips = lax.axis_size("x")
    top_count = expert_ids.shape[1]
    capacity = max(2, tok_rows * top_count * 5 // (4 * ep_count))
    half = capacity // CORES
    place = jnp.stack([lax.axis_index("x"), lax.axis_index("c")]).astype(jnp.int32)
    gate0, up0, down0 = gate_weight[0], up_weight[0], down_weight[0]
    both = lax.all_gather(prepare(in_hbm(tokens), in_hbm(pre_gain[None, :])), "c", axis=0)
    outgoing, cols = dispatch(
        place,
        both,
        in_hbm(jnp.transpose(expert_ids)),
        in_hbm(jnp.transpose(route_weights)),
        ep_count,
        capacity,
    )
    arrived = blocks_exchange(outgoing)
    swapped = []
    for weight in (gate0, up0, down0):
        swapped.append(swap(weight))
    arrived, gate1, up1, down1 = lax.optimization_barrier((arrived, *swapped))
    offsets, features = neighbours(arrange(arrived, both, half))
    squares = squares_of(features[:-1])
    hidden = hidden_of(place, squares, offsets, features, (gate0, up0, gate1, up1))
    *early, (last, hidden) = ring(hidden)
    summed = down_early(place, early, last, down0, down1, chips)
    result = down_last(summed, hidden, half)
    mixed = lax.all_gather(combine(blocks_exchange(result), cols), "c", axis=0)
    mixed, sums = sums_of(place, mixed, chips)
    sums = exchange(sums, "x")
    return final(mixed, sums, post_gain[None, :])


def solution(mesh):
    ep_count, tp_count = mesh.devices.shape
    devices = mesh.devices.reshape(ep_count, tp_count // CORES, CORES)
    return jax.shard_map(
        layer,
        mesh=Mesh(devices, ("ep", "x", "c")),
        in_specs=(
            P("ep", ("x", "c")),
            P("ep", None),
            P("ep", None),
            P(("x", "c")),
            P(("x", "c")),
            P("ep", None, ("x", "c")),
            P("ep", None, ("x", "c")),
            P("ep", None, ("x", "c")),
        ),
        out_specs=P("ep", ("x", "c")),
        check_vma=False,
    )
```
